512 devices in a mesh: sp: 64 (over z, y), tp: 8 (over x, core).
Axes of the slice: x: 4, y: 8, z: 8, core: 2. Of those that a mesh axis runs over, the one named last changes fastest.
Arguments:
- resid: bfloat16 [32768, 2048], P('sp'), may hold values from -6 to 6
- queries: bfloat16 [32768, 2048], P('sp', 'tp'), may hold values from -6 to 6
- keys: bfloat16 [32768, 512], P('sp', 'tp'), may hold values from -6 to 6
- values: bfloat16 [32768, 512], P('sp', 'tp'), may hold values from -6 to 6
- documents: int32 [32768], P('sp'), may hold values from 0 to 31, never falling along the last dimension, each value on 1 to 2048 neighbouring positions
- q_gain: float32 [64], replicated, may hold values from 0.5 to 6.5
- k_gain: float32 [64], replicated, may hold values from 0.5 to 6.5
- sink: float32 [32], P('tp'), may hold values from -1 to 5
- w_out: bfloat16 [2048, 2048], P('tp'), may hold values from -0.5 to 0.5
- n_gain: float32 [2048], replicated, may hold values from 0.1 to 1.9
- w_up: bfloat16 [2048, 8192], P('sp', 'tp'), may hold values from -0.125 to 0.125
- w_down: bfloat16 [8192, 2048], P('tp', 'sp'), may hold values from -0.0625 to 0.0625
Outputs:
- layer_out: bfloat16 [32768, 2048], P('sp')
The draws below stay inside these ranges and needn't reach their ends.
All inputs are finite; a program needn't handle non-finite values.
Results may differ from the reference program's by a relative error of at most 0.018.
The reference program's roundings to bfloat16 on the way count: a program that leaves them out, or rounds other values in their place, can miss the bound.
Values may be sent and summed in bfloat16 or wider, within the bound.
No kernel may reach another device: no remote copies, remote signals or barrier semaphores. Data moves between devices by JAX's collectives and lax.ppermute only.
A program may use at most 64 MiB of HBM per device.

```python
import math
import jax
import jax.numpy as jnp
import numpy as np
from jax import lax

D = 2048
HEADS = 32
KV_HEADS = 8
HEAD = 64
FF = 8192
WINDOW = 128
TOK_DEV = 512
TOKENS = 32768
N_SP = 64
N_TP = 8


def base_keys(key):
    return jax.random.normal(jax.random.fold_in(key, 3), (TOKENS, KV_HEADS * HEAD), jnp.float32)


def draw_keys(key, part):
    drawn = base_keys(key)
    return jnp.clip(drawn, -6.0, 6.0).astype(jnp.bfloat16)


def draw_queries(key, part):
    drawn = jax.random.normal(jax.random.fold_in(key, 7), (TOKENS, HEADS * HEAD), jnp.float32)
    return jnp.clip(drawn, -6.0, 6.0).astype(jnp.bfloat16)


def draw_q_gain(key, part):
    return jax.random.uniform(jax.random.fold_in(key, 21), (HEAD,), jnp.float32, 0.5, 1.5)


def draw_k_gain(key, part):
    return jax.random.uniform(jax.random.fold_in(key, 23), (HEAD,), jnp.float32, 0.5, 1.5)


def block_levels(key, shape, cuts, least, top_value):
    level, own = 1.0, jax.random.fold_in(key, 6)
    for position, shards_of in cuts:
        draws = jnp.exp(jax.random.uniform(jax.random.fold_in(own, position), (shards_of,), jnp.float32, least / len(cuts), top_value / len(cuts)))
        level = level * jnp.repeat(draws, shape[position] // shards_of).reshape([-1 if axis == position else 1 for axis in range(len(shape))])
    return level


def profile(number_of, total, bound, lean):
    loads = [(1 << 20) // math.isqrt(rank ** lean) + 1 for rank in range(2, number_of + 1)]
    rest, holding = total - bound - (number_of - 1), [1] * (number_of - 1)
    while rest > 0:
        candidates = [i for i in range(number_of - 1) if holding[i] < bound]
        mass, budget = sum([loads[i] for i in candidates]), rest
        for i in candidates:
            extra = min(bound - holding[i], max(1, budget * loads[i] // mass), rest)
            holding[i] = holding[i] + extra
            rest = rest - extra
    return np.array([bound] + holding)


def uneven(key, amount, total, limit, lean):
    if amount == 2:
        one = jax.random.randint(key, (), max(1, total - limit), min(limit, total - 1) + 1)
        return jnp.stack([one, total - one])
    sizes = jnp.asarray(profile(amount, total, limit, lean), jnp.int32)
    twos = (amount - 1) // 2
    source_of, taker = sizes[1:1 + 2 * twos:2], sizes[2:2 + 2 * twos:2]
    slack = jnp.minimum(source_of - 1, limit - taker)
    passed = jax.random.randint(jax.random.fold_in(key, 1), (twos,), 0, 1 << 20) % (slack + 1)
    sizes = sizes.at[1:1 + 2 * twos:2].set(source_of - passed).at[2:2 + 2 * twos:2].set(taker + passed)
    return sizes[jax.random.permutation(jax.random.fold_in(key, 2), amount)]


def gaussian(stream_key, extent, deviation, bound, cuts=(), kind=jnp.bfloat16):
    result = jax.random.normal(stream_key, extent, jnp.float32) * deviation
    if len(cuts) > 0:
        result = block_levels(stream_key, extent, cuts, -0.22, 0.18) * result
    return jnp.clip(result, min=-bound, max=bound).astype(kind)


def setup_inputs(seed: int = 0) -> dict:
    splits = jax.random.split(jax.random.key(seed), 13)
    resid = gaussian(splits[0], (TOKENS, D), 1.0, 6.0, ((0, 64),))
    queries = draw_queries(jax.random.fold_in(splits[12], 71), 0)
    keys = draw_keys(jax.random.fold_in(splits[12], 71), 0)
    values = gaussian(splits[3], (TOKENS, KV_HEADS * HEAD), 1.0, 6.0, ((0, 64), (1, 8)))
    documents = jnp.searchsorted(jnp.cumsum(uneven(splits[4], N_SP // 2, TOKENS, 4 * TOK_DEV, 0)), jnp.arange(TOKENS), side="right").astype(jnp.int32)
    q_gain = draw_q_gain(jax.random.fold_in(splits[12], 71), 0)
    k_gain = draw_k_gain(jax.random.fold_in(splits[12], 71), 0)
    sink = jnp.clip(-1.0 + 6.0 * jax.random.uniform(splits[7], (HEADS,), jnp.float32) ** block_levels(splits[7], (HEADS,), ((0, 8),), -0.2, 0.2), -1.0, 5.0)
    w_out = gaussian(splits[8], (HEADS * HEAD, D), (HEADS * HEAD // 16) ** -0.5, 0.5, ((0, 8),))
    n_gain = jnp.clip(1.0 + 0.18 * jax.random.normal(splits[9], (D,), jnp.float32), 0.1, 1.9)
    w_up = gaussian(splits[10], (D, FF), D ** -0.5, 0.125, ((0, 64), (1, 8)))
    w_down = gaussian(splits[11], (FF, D), FF ** -0.5, 0.0625, ((0, 8), (1, 64)))
    return dict(resid=resid, queries=queries, keys=keys, values=values, documents=documents, q_gain=q_gain, k_gain=k_gain, sink=sink, w_out=w_out, n_gain=n_gain, w_up=w_up, w_down=w_down)


EPS = 1e-06

def rms_scale(field, gain):
    wide = field.astype(jnp.float32)
    return wide * lax.rsqrt(lax.optimization_barrier(jnp.mean(wide * wide, axis=-1, keepdims=True)) + EPS) * gain.astype(jnp.float32)

def reference(resid, queries, keys, values, documents, q_gain, k_gain, sink, w_out, n_gain, w_up, w_down):
    group = HEADS // KV_HEADS
    qnorm = rms_scale(queries.reshape(TOKENS, KV_HEADS, group, HEAD), q_gain).astype(jnp.bfloat16)
    knorm = rms_scale(keys.reshape(TOKENS, KV_HEADS, HEAD), k_gain).astype(jnp.bfloat16)
    vheads = values.reshape(TOKENS, KV_HEADS, HEAD)
    padding = ((WINDOW, WINDOW), (0, 0), (0, 0))
    key_pad = jnp.pad(knorm, padding)
    value_pad = jnp.pad(vheads, padding)
    doc_pad = jnp.pad(documents, (WINDOW, WINDOW), constant_values=-1)
    slopes = jnp.exp2(-8.0 * (jnp.arange(HEADS, dtype=jnp.float32) + 1.0) / HEADS).reshape(KV_HEADS, group)
    sink_f = sink.astype(jnp.float32).reshape(KV_HEADS, group)
    span = TOK_DEV
    blocks = TOKENS // span
    query_blocks = qnorm.reshape(blocks, span, KV_HEADS, group, HEAD)
    doc_blocks = documents.reshape(blocks, span)

    def one_block(args):
        qblock, dblock, number = args
        start = number * span
        kblock = lax.dynamic_slice_in_dim(key_pad, start, span + 2 * WINDOW, 0)
        vblock = lax.dynamic_slice_in_dim(value_pad, start, span + 2 * WINDOW, 0)
        dkeys = lax.dynamic_slice_in_dim(doc_pad, start, span + 2 * WINDOW, 0)
        query_pos = start + jnp.arange(span, dtype=jnp.int32)
        key_pos = start - WINDOW + jnp.arange(span + 2 * WINDOW, dtype=jnp.int32)
        distance = key_pos[None, :] - query_pos[:, None]
        allowed = (jnp.abs(distance) <= WINDOW) & (key_pos[None, :] >= 0) & (key_pos[None, :] < TOKENS)
        allowed = allowed & (dkeys[None, :] == dblock[:, None])
        scores = jnp.einsum('rkgd,skd->kgrs', qblock.astype(jnp.float32), kblock.astype(jnp.float32)) * HEAD ** (-0.5)
        scores = scores - slopes[:, :, None, None] * jnp.abs(distance).astype(jnp.float32)[None, None]
        scores = jnp.where(allowed[None, None], scores, jnp.float32(-1e+30))
        highest = jnp.maximum(lax.optimization_barrier(jnp.max(scores, axis=-1)), sink_f[:, :, None])
        weights = jnp.exp(scores - highest[..., None])
        denom = lax.optimization_barrier(jnp.sum(weights, axis=-1)) + jnp.exp(sink_f[:, :, None] - highest)
        rounded = weights.astype(jnp.bfloat16)
        summed = jnp.einsum('kgrs,skd->rkgd', rounded.astype(jnp.float32), vblock.astype(jnp.float32))
        return (summed / denom.transpose(2, 0, 1)[..., None]).astype(jnp.bfloat16)
    attended = lax.map(one_block, (query_blocks, doc_blocks, jnp.arange(blocks, dtype=jnp.int32)))
    attended = attended.reshape(TOKENS, HEADS * HEAD)
    cols = HEADS * HEAD // N_TP
    head_mix = jnp.zeros((TOKENS, D), jnp.float32)
    for index in range(N_TP):
        partial_sum = jnp.dot(attended[:, index * cols:(index + 1) * cols], w_out[index * cols:(index + 1) * cols], preferred_element_type=jnp.float32)
        head_mix = head_mix + partial_sum.astype(jnp.bfloat16).astype(jnp.float32)
    middle = (resid.astype(jnp.float32) + head_mix).astype(jnp.bfloat16)
    normed = rms_scale(middle, n_gain).astype(jnp.bfloat16)
    units = FF // N_TP
    unit_mix = jnp.zeros((TOKENS, D), jnp.float32)
    for index in range(N_TP):
        upward = jnp.dot(normed, w_up[:, index * units:(index + 1) * units], preferred_element_type=jnp.float32)
        active = jnp.square(jax.nn.relu(upward)).astype(jnp.bfloat16)
        partial_sum = jnp.dot(active, w_down[index * units:(index + 1) * units], preferred_element_type=jnp.float32)
        unit_mix = unit_mix + partial_sum.astype(jnp.bfloat16).astype(jnp.float32)
    return (middle.astype(jnp.float32) + unit_mix).astype(jnp.bfloat16)
```

```python
import jax
import jax.numpy as jnp
from jax import lax
from jax.sharding import Mesh
from jax.sharding import PartitionSpec as P

WINDOW = 128
EPS = 1e-06
SP = ("z", "y")
TP = ("x", "c")


def shift(x, axis, by):
    n = lax.axis_size(axis)
    return lax.ppermute(x, axis, [(i, (i + by) % n) for i in range(n)])


def swap(x):
    return lax.ppermute(x, "c", [(0, 1), (1, 0)])


def extended(x, width):
    count, length = lax.axis_size("z") * lax.axis_size("y"), x.shape[0]
    up = [(i, (i + 1) % count) for i in range(count - 1)]
    down = [(j, i) for i, j in up]
    before = lax.ppermute(x[length - width :], SP, up)
    after = lax.ppermute(x[:width], SP, down)
    return jnp.concatenate([before, x, after], axis=0)


def rms_scale(field, gain):
    wide = field.astype(jnp.float32)
    return wide * lax.rsqrt(jnp.mean(wide * wide, axis=-1, keepdims=True) + EPS) * gain


def scatter_x(x):
    n = lax.axis_size("x")
    tiles = lax.all_to_all(x.reshape(n, x.shape[0] // n, x.shape[1]), "x", 0, 0, tiled=True)
    return jnp.sum(tiles.astype(jnp.float32), axis=0)


def gather_x(x):
    n = lax.axis_size("x")
    tiles = lax.all_to_all(jnp.broadcast_to(x, (n, *x.shape)), "x", 0, 0, tiled=True)
    return tiles.reshape(n * x.shape[0], x.shape[1])


def mixer(normed, up, down_t):
    upward = jnp.dot(normed, up, preferred_element_type=jnp.float32)
    active = jnp.square(jax.nn.relu(upward)).astype(jnp.bfloat16)
    return lax.dot_general(
        active, down_t, (((1,), (1,)), ((), ())), preferred_element_type=jnp.float32
    )


def shards(
    resid, queries, keys, values, documents, q_gain, k_gain, sink, w_out, n_gain, w_up, w_down
):
    rows = resid.shape[0]
    head_size = q_gain.shape[0]
    heads_here = sink.shape[0]
    kv_here = keys.shape[1] // head_size
    group = heads_here // kv_here
    core = lax.axis_index("c")
    units = w_up.shape[1]
    both = lax.all_gather(jnp.concatenate([w_up, w_down.T], axis=1), SP, axis=0, tiled=True)
    w_out_other = swap(w_out)
    qnorm = rms_scale(queries.reshape(rows, kv_here, group, head_size), q_gain).astype(jnp.bfloat16)
    knorm = rms_scale(keys.reshape(rows, kv_here, head_size), k_gain).astype(jnp.bfloat16)
    vheads = values.reshape(rows, kv_here, head_size)
    doc_here = documents.astype(jnp.bfloat16)
    near_keys = extended(knorm, WINDOW)
    near_values = extended(vheads, WINDOW)
    near_docs = extended(doc_here, WINDOW)
    offset = lax.axis_index(SP) * rows
    total = rows * lax.axis_size(SP)
    query_pos = offset + jnp.arange(rows, dtype=jnp.int32)
    key_pos = offset - WINDOW + jnp.arange(rows + 2 * WINDOW, dtype=jnp.int32)
    distance = key_pos[None, :] - query_pos[:, None]
    allowed = (jnp.abs(distance) <= WINDOW) & (key_pos[None, :] >= 0) & (key_pos[None, :] < total)
    allowed = allowed & (near_docs[None, :] == doc_here[:, None])
    heads_all = heads_here * lax.axis_size(TP)
    first_head = (lax.axis_index(TP) * heads_here).astype(jnp.float32)
    slopes = jnp.exp2(
        -8.0 * (first_head + jnp.arange(heads_here, dtype=jnp.float32) + 1.0) / heads_all
    )
    slopes = slopes.reshape(kv_here, group)
    sink_f = sink.reshape(kv_here, group)
    scores = jnp.einsum(
        "rkgd,skd->kgrs", qnorm, near_keys, preferred_element_type=jnp.float32
    ) * head_size ** (-0.5)
    scores = scores - slopes[:, :, None, None] * jnp.abs(distance).astype(jnp.float32)[None, None]
    scores = jnp.where(allowed[None, None], scores, jnp.float32(-1e30))
    highest = jnp.maximum(jnp.max(scores, axis=-1), sink_f[:, :, None])
    weights = jnp.exp(scores - highest[..., None])
    denom = jnp.sum(weights, axis=-1) + jnp.exp(sink_f[:, :, None] - highest)
    summed = jnp.einsum(
        "kgrs,skd->rkgd",
        weights.astype(jnp.bfloat16),
        near_values,
        preferred_element_type=jnp.float32,
    )
    attended = (
        (summed / denom.transpose(2, 0, 1)[..., None])
        .astype(jnp.bfloat16)
        .reshape(rows, heads_here * head_size)
    )
    half = rows // 2
    share = rows // lax.axis_size(TP)
    att_own = lax.dynamic_slice_in_dim(attended, core * half, half, 0)
    att_other = swap(lax.dynamic_slice_in_dim(attended, (1 - core) * half, half, 0))
    partial = jnp.dot(att_own, w_out, preferred_element_type=jnp.float32) + jnp.dot(
        att_other, w_out_other, preferred_element_type=jnp.float32
    )
    head_mix = scatter_x(partial.astype(jnp.bfloat16))
    start = core * half + lax.axis_index("x") * share
    own_resid = lax.dynamic_slice_in_dim(resid, start, share, 0)
    middle = (own_resid.astype(jnp.float32) + head_mix).astype(jnp.bfloat16)
    normed = gather_x(rms_scale(middle, n_gain).astype(jnp.bfloat16))
    normed_other = swap(normed)
    up, down_t = both[:, :units], both[:, units:]
    sent = swap(mixer(normed_other, up, down_t).astype(jnp.bfloat16))
    partial_sum = mixer(normed, up, down_t) + sent.astype(jnp.float32)
    unit_mix = scatter_x(partial_sum.astype(jnp.bfloat16))
    finished = gather_x((middle.astype(jnp.float32) + unit_mix).astype(jnp.bfloat16))
    finished_other = swap(finished)
    low = jnp.where(core == 0, finished, finished_other)
    high = jnp.where(core == 0, finished_other, finished)
    return jnp.concatenate([low, high], axis=0)


def solution(mesh):
    fine = Mesh(mesh.devices.reshape(8, 8, 4, 2), ("z", "y", "x", "c"))
    placed = (
        P(SP, None),
        P(SP, TP),
        P(SP, TP),
        P(SP, TP),
        P(SP),
        P(),
        P(),
        P(TP),
        P(TP, None),
        P(),
        P(SP, TP),
        P(TP, SP),
    )
    return jax.shard_map(
        shards, mesh=fine, in_specs=placed, out_specs=P(SP, None), check_vma=False
    )
```

```python
import jax
import jax.numpy as jnp
from jax import lax
from jax.experimental import pallas as pl
from jax.experimental.pallas import tpu as pltpu
from jax.sharding import Mesh
from jax.sharding import PartitionSpec as P

WINDOW = 128
EPS = 1e-06
SP = ("z", "y")
TP = ("x", "c")


def shift(x, axis, by):
    n = lax.axis_size(axis)
    return lax.ppermute(x, axis, [(i, (i + by) % n) for i in range(n)])


def swap(x):
    return lax.ppermute(x, "c", [(0, 1), (1, 0)])


def spread(x, axis):
    n = lax.axis_size(axis)
    tiles = lax.all_to_all(jnp.broadcast_to(x, (n, *x.shape)), axis, 0, 0, tiled=True)
    return tiles.reshape(n * x.shape[0], x.shape[1])


def ring(block, axis):
    n = lax.axis_size(axis)
    here = lax.axis_index(axis)
    size = block.shape[0]
    out = jnp.zeros((n * size, block.shape[1]), block.dtype)

    def put(out, piece, at, extra=0):
        return lax.dynamic_update_slice_in_dim(out, piece, (at % n) * size + extra, 0)

    out = put(out, block, here)
    up = down = block
    for k in range(1, n // 2):
        up, down = shift(up, axis, 1), shift(down, axis, -1)
        out = put(out, up, here - k + n)
        out = put(out, down, here + k)
    cut = size // 2
    out = put(out, shift(up[:cut], axis, 1), here + n // 2)
    return put(out, shift(down[cut:], axis, -1), here + n // 2, cut)


def rms_scale(field, gain):
    wide = field.astype(jnp.float32)
    return wide * lax.rsqrt(jnp.mean(wide * wide, axis=-1, keepdims=True) + EPS) * gain


def scatter_x(x):
    n = lax.axis_size("x")
    tiles = lax.all_to_all(x.reshape(n, x.shape[0] // n, x.shape[1]), "x", 0, 0, tiled=True)
    return jnp.sum(tiles.astype(jnp.float32), axis=0)


def attention_body(
    core_ref, slope_ref, sink_ref, q_ref, kt_ref, vt_ref, doc_ref, before_ref, after_ref,
    qg_ref, kg_ref, other_ref, own_ref, kn_ref, vn_ref, dk_ref
):
    head = kt_ref.shape[0]
    heads = q_ref.shape[1] // head
    kg = kg_ref[...]
    for j in range(6):
        if j == 0:
            kt, vt, doc = before_ref[:head, :], before_ref[head : 2 * head, :], before_ref[2 * head : 2 * head + 8, :]
        elif j == 5:
            kt, vt, doc = after_ref[:head, :], after_ref[head : 2 * head, :], after_ref[2 * head : 2 * head + 8, :]
        else:
            lanes = slice((j - 1) * WINDOW, j * WINDOW)
            kt, vt, doc = kt_ref[:, lanes], vt_ref[:, lanes], doc_ref[:8, lanes]
        wide = kt.astype(jnp.float32)
        scale = lax.rsqrt(jnp.mean(wide * wide, axis=0, keepdims=True) + EPS)
        kn_ref[j] = (wide * scale * kg).astype(jnp.bfloat16)
        vn_ref[j] = vt
        dk_ref[j] = doc.astype(jnp.float32)
    row = lax.broadcasted_iota(jnp.int32, (WINDOW, 3 * WINDOW), 0)
    col = lax.broadcasted_iota(jnp.int32, (WINDOW, 3 * WINDOW), 1)
    distance = jnp.abs(col - WINDOW - row)
    near = distance <= WINDOW
    far = distance.astype(jnp.float32)
    core = core_ref[0]
    for half in range(2):
        side = 1 - core if half == 0 else core
        for j in range(2):
            block = 2 * side + j
            q = q_ref[pl.ds(pl.multiple_of(block * WINDOW, WINDOW), WINDOW), :]
            keys = jnp.concatenate([kn_ref[block], kn_ref[block + 1], kn_ref[block + 2]], axis=1)
            vals = jnp.concatenate([vn_ref[block], vn_ref[block + 1], vn_ref[block + 2]], axis=1)
            doc_k = jnp.concatenate(
                [jnp.broadcast_to(dk_ref[block + i][:1], (WINDOW, WINDOW)) for i in range(3)], axis=1
            )
            doc_q = jnp.broadcast_to(dk_ref[block + 1][:1], (WINDOW, WINDOW)).T
            allowed = near & (doc_k == jnp.concatenate([doc_q] * 3, axis=1))
            outs = []
            for h in range(heads):
                wide = q[:, h * head : (h + 1) * head].astype(jnp.float32)
                scale = lax.rsqrt(jnp.mean(wide * wide, axis=-1, keepdims=True) + EPS)
                qn = (wide * scale * qg_ref[...]).astype(jnp.bfloat16)
                s = jnp.dot(qn, keys, preferred_element_type=jnp.float32) * head ** (-0.5)
                s = jnp.where(allowed, s - slope_ref[h] * far, jnp.float32(-1e30))
                top = jnp.maximum(jnp.max(s, axis=-1, keepdims=True), sink_ref[h])
                p = jnp.exp(s - top)
                denom = jnp.sum(p, axis=-1, keepdims=True) + jnp.exp(sink_ref[h] - top)
                mixed = lax.dot_general(
                    p.astype(jnp.bfloat16), vals, (((1,), (1,)), ((), ())),
                    preferred_element_type=jnp.float32,
                )
                outs.append((mixed / denom).astype(jnp.bfloat16))
            target = other_ref if half == 0 else own_ref
            target[j * WINDOW : (j + 1) * WINDOW, :] = jnp.concatenate(outs, axis=1)


def attention(core, slopes, sink, q, kt, vt, doc, before, after, q_gain, k_gain):
    head, rows = kt.shape
    smem = pl.BlockSpec(memory_space=pltpu.SMEM)
    vmem = pl.BlockSpec(memory_space=pltpu.VMEM)
    out = jax.ShapeDtypeStruct((rows // 2, q.shape[1]), jnp.bfloat16)
    return pl.pallas_call(
        attention_body,
        in_specs=[smem] * 3 + [vmem] * 8,
        out_specs=[vmem, vmem],
        out_shape=[out, out],
        scratch_shapes=[
            pltpu.VMEM((6, head, WINDOW), jnp.bfloat16),
            pltpu.VMEM((6, head, WINDOW), jnp.bfloat16),
            pltpu.VMEM((6, 8, WINDOW), jnp.float32),
        ],
        cost_estimate=pl.CostEstimate(flops=1 << 31, transcendentals=1 << 20, bytes_accessed=1 << 20),
        name="attend",
    )(core, slopes, sink, q, kt, vt, doc, before, after, q_gain, k_gain)


def shards(
    resid, queries, keys, values, documents, q_gain, k_gain, sink, w_out, n_gain, w_up, w_down
):
    rows = resid.shape[0]
    heads_here = sink.shape[0]
    core = lax.axis_index("c")
    half = rows // 2
    share = rows // lax.axis_size(TP)

    up_part = spread(w_up, "z")
    down_part = spread(w_down.T, "y")
    up = lax.all_gather(up_part, "y", axis=0, tiled=True)
    down_t = ring(down_part, "z")

    kt, vt = keys.T, values.T
    doc = jnp.broadcast_to((documents + 1).astype(jnp.bfloat16)[None, :], (16, rows))
    packed = jnp.concatenate([kt, vt, doc], axis=0)
    count = lax.axis_size(SP)
    onward = [(i, i + 1) for i in range(count - 1)]
    before = lax.ppermute(packed[:, rows - WINDOW :], SP, onward)
    after = lax.ppermute(packed[:, :WINDOW], SP, [(j, i) for i, j in onward])
    w_out_other = swap(w_out)

    heads_all = heads_here * lax.axis_size(TP)
    first_head = (lax.axis_index(TP) * heads_here).astype(jnp.float32)
    slopes = jnp.exp2(
        -8.0 * (first_head + jnp.arange(heads_here, dtype=jnp.float32) + 1.0) / heads_all
    )
    att_send, att_own = attention(
        core.astype(jnp.int32).reshape(1), slopes, sink, queries, kt, vt, doc, before, after,
        q_gain[None, :], k_gain[:, None],
    )
    att_other = swap(att_send)
    partial = jnp.dot(att_own, w_out, preferred_element_type=jnp.float32) + jnp.dot(
        att_other, w_out_other, preferred_element_type=jnp.float32
    )
    head_mix = scatter_x(partial.astype(jnp.bfloat16))
    start = core * half + lax.axis_index("x") * share
    own_resid = lax.dynamic_slice_in_dim(resid, start, share, 0)
    middle = (own_resid.astype(jnp.float32) + head_mix).astype(jnp.bfloat16)
    normed = rms_scale(middle, n_gain).astype(jnp.bfloat16)
    nz, ny = lax.axis_size("z"), lax.axis_size("y")
    turned = normed.reshape(share, nz, ny, -1).swapaxes(1, 2).reshape(normed.shape)
    mine = spread(turned, "x")
    normed_all = jnp.concatenate([swap(mine), mine], axis=0)

    upward = jnp.dot(normed_all, up, preferred_element_type=jnp.float32)
    active = jnp.square(jax.nn.relu(upward)).astype(jnp.bfloat16)
    dims = (((1,), (1,)), ((), ()))
    sent = swap(
        lax.dot_general(active[:half], down_t, dims, preferred_element_type=jnp.float32).astype(
            jnp.bfloat16
        )
    )
    kept = lax.dot_general(active[half:], down_t, dims, preferred_element_type=jnp.float32)
    unit_mix = scatter_x((kept + sent.astype(jnp.float32)).astype(jnp.bfloat16))
    finished = spread((middle.astype(jnp.float32) + unit_mix).astype(jnp.bfloat16), "x")
    finished_other = swap(finished)
    low = jnp.where(core == 0, finished, finished_other)
    high = jnp.where(core == 0, finished_other, finished)
    return jnp.concatenate([low, high], axis=0)


def solution(mesh):
    fine = Mesh(mesh.devices.reshape(8, 8, 4, 2), ("z", "y", "x", "c"))
    placed = (
        P(SP, None),
        P(SP, TP),
        P(SP, TP),
        P(SP, TP),
        P(SP),
        P(),
        P(),
        P(TP),
        P(TP, None),
        P(),
        P(SP, TP),
        P(TP, SP),
    )
    return jax.shard_map(
        shards, mesh=fine, in_specs=placed, out_specs=P(SP, None), check_vma=False
    )
```

```python
import jax
import jax.numpy as jnp
from jax import lax
from jax.experimental import pallas as pl
from jax.experimental.pallas import tpu as pltpu
from jax.sharding import Mesh
from jax.sharding import PartitionSpec as P

WINDOW = 128
EPS = 1e-06
SP = ("z", "y")
TP = ("x", "c")


def shift(x, axis, by):
    n = lax.axis_size(axis)
    return lax.ppermute(x, axis, [(i, (i + by) % n) for i in range(n)])


def swap(x):
    return lax.ppermute(x, "c", [(0, 1), (1, 0)])


def spread(x, axis):
    n = lax.axis_size(axis)
    tiles = lax.all_to_all(jnp.broadcast_to(x, (n, *x.shape)), axis, 0, 0, tiled=True)
    return tiles.reshape(n * x.shape[0], x.shape[1])


def tie(x, y):
    return lax.optimization_barrier((x, y))[0]


def down_body(z_ref, act_ref, *refs):
    *pieces, out_ref = refs
    act = act_ref[...]
    dims = (((1,), (1,)), ((), ()))
    blocks = out_ref.shape[1]
    for r in range(blocks):
        if r < blocks // 2:
            piece = pieces[r][...]
        elif r > blocks // 2:
            piece = pieces[r + 1][...]
        else:
            piece = jnp.concatenate([pieces[r][...], pieces[r + 1][...]], axis=0)
        done = lax.dot_general(act, piece, dims, preferred_element_type=jnp.float32)
        at = lax.rem(z_ref[0] + r, blocks)
        out_ref[:, at] = done.astype(out_ref.dtype).reshape(
            out_ref.shape[0], out_ref.shape[2], out_ref.shape[3]
        )


def down(z, act, pieces, share):
    size = pieces[0].shape[0]
    smem = pl.BlockSpec(memory_space=pltpu.SMEM)
    vmem = pl.BlockSpec(memory_space=pltpu.VMEM)
    return pl.pallas_call(
        down_body,
        in_specs=[smem] + [vmem] * (1 + len(pieces)),
        out_specs=vmem,
        out_shape=jax.ShapeDtypeStruct(
            (act.shape[0] // share, len(pieces) - 1, share, size), jnp.bfloat16
        ),
        cost_estimate=pl.CostEstimate(flops=1 << 30, transcendentals=0, bytes_accessed=1 << 23),
        compiler_params=pltpu.CompilerParams(vmem_limit_bytes=40 << 20),
        name="down",
    )(z, act, *pieces)


def rms_scale(field, gain):
    wide = field.astype(jnp.float32)
    return wide * lax.rsqrt(jnp.mean(wide * wide, axis=-1, keepdims=True) + EPS) * gain


def attention_body(
    core_ref, slope_ref, sink_ref, q_ref, kt_ref, vt_ref, doc_ref, before_ref, after_ref,
    qg_ref, kg_ref, other_ref, own_ref, kn_ref, vn_ref, dk_ref
):
    head = kt_ref.shape[0]
    heads = q_ref.shape[1] // head
    kg = kg_ref[...]
    for j in range(6):
        if j == 0:
            kt, vt, doc = before_ref[:head, :], before_ref[head : 2 * head, :], before_ref[2 * head : 2 * head + 8, :]
        elif j == 5:
            kt, vt, doc = after_ref[:head, :], after_ref[head : 2 * head, :], after_ref[2 * head : 2 * head + 8, :]
        else:
            lanes = slice((j - 1) * WINDOW, j * WINDOW)
            kt, vt, doc = kt_ref[:, lanes], vt_ref[:, lanes], doc_ref[:8, lanes]
        wide = kt.astype(jnp.float32)
        scale = lax.rsqrt(jnp.mean(wide * wide, axis=0, keepdims=True) + EPS)
        kn_ref[j] = (wide * scale * kg).astype(jnp.bfloat16)
        vn_ref[j] = vt
        dk_ref[j] = doc.astype(jnp.float32)
    row = lax.broadcasted_iota(jnp.int32, (WINDOW, 3 * WINDOW), 0)
    col = lax.broadcasted_iota(jnp.int32, (WINDOW, 3 * WINDOW), 1)
    distance = jnp.abs(col - WINDOW - row)
    near = distance <= WINDOW
    far = distance.astype(jnp.float32)
    core = core_ref[0]
    for half in range(2):
        side = 1 - core if half == 0 else core
        for j in range(2):
            block = 2 * side + j
            q = q_ref[pl.ds(pl.multiple_of(block * WINDOW, WINDOW), WINDOW), :]
            keys = jnp.concatenate([kn_ref[block], kn_ref[block + 1], kn_ref[block + 2]], axis=1)
            vals = jnp.concatenate([vn_ref[block], vn_ref[block + 1], vn_ref[block + 2]], axis=1)
            doc_k = jnp.concatenate(
                [jnp.broadcast_to(dk_ref[block + i][:1], (WINDOW, WINDOW)) for i in range(3)], axis=1
            )
            doc_q = jnp.broadcast_to(dk_ref[block + 1][:1], (WINDOW, WINDOW)).T
            allowed = near & (doc_k == jnp.concatenate([doc_q] * 3, axis=1))
            outs = []
            for h in range(heads):
                wide = q[:, h * head : (h + 1) * head].astype(jnp.float32)
                scale = lax.rsqrt(jnp.mean(wide * wide, axis=-1, keepdims=True) + EPS)
                qn = (wide * scale * qg_ref[...]).astype(jnp.bfloat16)
                s = jnp.dot(qn, keys, preferred_element_type=jnp.float32) * head ** (-0.5)
                s = jnp.where(allowed, s - slope_ref[h] * far, jnp.float32(-1e30))
                top = jnp.maximum(jnp.max(s, axis=-1, keepdims=True), sink_ref[h])
                p = jnp.exp(s - top)
                denom = jnp.sum(p, axis=-1, keepdims=True) + jnp.exp(sink_ref[h] - top)
                mixed = lax.dot_general(
                    p.astype(jnp.bfloat16), vals, (((1,), (1,)), ((), ())),
                    preferred_element_type=jnp.float32,
                )
                outs.append((mixed / denom).astype(jnp.bfloat16))
            target = other_ref if half == 0 else own_ref
            target[j * WINDOW : (j + 1) * WINDOW, :] = jnp.concatenate(outs, axis=1)


def attention(core, slopes, sink, q, kt, vt, doc, before, after, q_gain, k_gain):
    head, rows = kt.shape
    smem = pl.BlockSpec(memory_space=pltpu.SMEM)
    vmem = pl.BlockSpec(memory_space=pltpu.VMEM)
    out = jax.ShapeDtypeStruct((rows // 2, q.shape[1]), jnp.bfloat16)
    return pl.pallas_call(
        attention_body,
        in_specs=[smem] * 3 + [vmem] * 8,
        out_specs=[vmem, vmem],
        out_shape=[out, out],
        scratch_shapes=[
            pltpu.VMEM((6, head, WINDOW), jnp.bfloat16),
            pltpu.VMEM((6, head, WINDOW), jnp.bfloat16),
            pltpu.VMEM((6, 8, WINDOW), jnp.float32),
        ],
        cost_estimate=pl.CostEstimate(flops=1 << 31, transcendentals=1 << 20, bytes_accessed=1 << 20),
        name="attend",
    )(core, slopes, sink, q, kt, vt, doc, before, after, q_gain, k_gain)


def shards(
    resid, queries, keys, values, documents, q_gain, k_gain, sink, w_out, n_gain, w_up, w_down
):
    rows = resid.shape[0]
    heads_here = sink.shape[0]
    core = lax.axis_index("c")
    half = rows // 2
    share = rows // lax.axis_size(TP)
    nx = lax.axis_size("x")

    up = lax.all_gather(w_up, SP, axis=0, tiled=True)

    kt, vt = keys.T, values.T
    doc = jnp.broadcast_to((documents + 1).astype(jnp.bfloat16)[None, :], (16, rows))
    packed = jnp.concatenate([kt, vt, doc], axis=0)
    count = lax.axis_size(SP)
    onward = [(i, i + 1) for i in range(count - 1)]
    before = lax.ppermute(packed[:, rows - WINDOW :], SP, onward)
    after = lax.ppermute(packed[:, :WINDOW], SP, [(j, i) for i, j in onward])
    piece = spread(tie(w_down.T, packed), "y")
    w_out_other = swap(w_out)

    heads_all = heads_here * lax.axis_size(TP)
    first_head = (lax.axis_index(TP) * heads_here).astype(jnp.float32)
    slopes = jnp.exp2(
        -8.0 * (first_head + jnp.arange(heads_here, dtype=jnp.float32) + 1.0) / heads_all
    )
    att_send, att_own = attention(
        core.astype(jnp.int32).reshape(1), slopes, sink, queries, kt, vt, doc, before, after,
        q_gain[None, :], k_gain[:, None],
    )
    piece = tie(piece, att_send)
    cut = piece.shape[0] // 2
    up1, dn1 = shift(piece, "z", 1), shift(piece, "z", -1)
    up2, dn2 = shift(up1, "z", 1), shift(dn1, "z", -1)
    up3, dn3 = shift(up2, "z", 1), shift(dn2, "z", -1)
    up4, dn4 = shift(up3[:cut], "z", 1), shift(dn3[cut:], "z", -1)
    pieces = [piece, dn1, dn2, dn3, up4, dn4, up3, up2, up1]

    att_other = swap(att_send)
    partial = jnp.dot(att_own, w_out, preferred_element_type=jnp.float32) + jnp.dot(
        att_other, w_out_other, preferred_element_type=jnp.float32
    )
    tiles = lax.all_to_all(
        partial.astype(jnp.bfloat16).reshape(nx, share, -1), "x", 0, 0, tiled=True
    )
    head_mix = jnp.sum(tiles.astype(jnp.float32), axis=0)
    start = core * half + lax.axis_index("x") * share
    own_resid = lax.dynamic_slice_in_dim(resid, start, share, 0)
    middle = (own_resid.astype(jnp.float32) + head_mix).astype(jnp.bfloat16)
    normed = rms_scale(middle, n_gain).astype(jnp.bfloat16)
    mine = spread(normed, "x")
    normed_all = jnp.concatenate([swap(mine), mine], axis=0)

    upward = jnp.dot(normed_all, up, preferred_element_type=jnp.float32)
    active = jnp.square(jax.nn.relu(upward)).astype(jnp.bfloat16)
    z = lax.axis_index("z").astype(jnp.int32).reshape(1)
    sent = swap(down(z, active[:half], pieces, share))
    kept = down(z, active[half:], pieces, share)
    joined = (kept.astype(jnp.float32) + sent.astype(jnp.float32)).astype(jnp.bfloat16)
    tiles = lax.all_to_all(joined, "x", 0, 0, tiled=True)
    unit_mix = jnp.sum(tiles.astype(jnp.float32), axis=0).swapaxes(0, 1).reshape(share, -1)
    finished = spread((middle.astype(jnp.float32) + unit_mix).astype(jnp.bfloat16), "x")
    finished_other = swap(finished)
    low = jnp.where(core == 0, finished, finished_other)
    high = jnp.where(core == 0, finished_other, finished)
    return jnp.concatenate([low, high], axis=0)


def solution(mesh):
    fine = Mesh(mesh.devices.reshape(8, 8, 4, 2), ("z", "y", "x", "c"))
    placed = (
        P(SP, None),
        P(SP, TP),
        P(SP, TP),
        P(SP, TP),
        P(SP),
        P(),
        P(),
        P(TP),
        P(TP, None),
        P(),
        P(SP, TP),
        P(TP, SP),
    )
    return jax.shard_map(shards, mesh=fine, in_specs=placed, out_specs=P(SP, None), check_vma=False)
```

```python
import jax
import jax.numpy as jnp
from jax import lax
from jax.experimental import pallas as pl
from jax.experimental.pallas import tpu as pltpu
from jax.sharding import Mesh
from jax.sharding import PartitionSpec as P

WINDOW = 128
EPS = 1e-06
SP = ("z", "y")
TP = ("x", "c")


def along(x, by):
    nz, ny = lax.axis_size("z"), lax.axis_size("y")
    pairs = []
    for z in range(nz):
        for y in range(ny):
            here = 2 * (z * ny + y)
            pairs.append((here, 2 * (z * ny + (y + by) % ny)))
            pairs.append((here + 1, 2 * ((z + by) % nz * ny + y) + 1))
    return lax.ppermute(x, ("z", "y", "c"), pairs)


def across(x):
    nz, ny = lax.axis_size("z"), lax.axis_size("y")
    groups = [[2 * (z * ny + y) for z in range(nz)] for y in range(ny)]
    groups += [[2 * (z * ny + y) + 1 for y in range(ny)] for z in range(nz)]
    tiles = lax.all_to_all(
        jnp.broadcast_to(x, (nz, *x.shape)),
        ("z", "y", "c"), 0, 0, tiled=True, axis_index_groups=groups,
    )
    return tiles.reshape(nz * x.shape[0], x.shape[1])


def swap(x):
    return lax.ppermute(x, "c", [(0, 1), (1, 0)])


def spread(x, axis):
    n = lax.axis_size(axis)
    tiles = lax.all_to_all(jnp.broadcast_to(x, (n, *x.shape)), axis, 0, 0, tiled=True)
    return tiles.reshape(n * x.shape[0], x.shape[1])


def tie(x, y):
    return lax.optimization_barrier((x, y))[0]


def scatter_x(x):
    n = lax.axis_size("x")
    tiles = lax.all_to_all(x.reshape(n, x.shape[0] // n, x.shape[1]), "x", 0, 0, tiled=True)
    return jnp.sum(tiles.astype(jnp.float32), axis=0)


def rms_scale(field, gain):
    wide = field.astype(jnp.float32)
    return wide * lax.rsqrt(jnp.mean(wide * wide, axis=-1, keepdims=True) + EPS) * gain


def mixer_body(at_ref, theirs_ref, mine_ref, *refs):
    *pieces, down_ref, act_ref, out_ref, up_ref = refs
    count = len(pieces) - 1
    units = act_ref.shape[1]
    cut = pieces[count // 2].shape[0]
    chunk = 2 * cut // count
    for r in range(count):
        index = lax.rem(at_ref[0] + r, count)
        for j in range(count):
            if r < count // 2:
                source, low = pieces[r], j * chunk
            elif r > count // 2:
                source, low = pieces[r + 1], j * chunk
            else:
                source, low = pieces[r + j * chunk // cut], j * chunk % cut
            to = pl.multiple_of(j * at_ref[1] + index * at_ref[2], chunk)
            up_ref[pl.ds(to, chunk), :] = source[low : low + chunk, :units]
            down_ref[pl.ds(to, chunk), :] = source[low : low + chunk, units:]

    def hidden(rows):
        wide = jnp.dot(rows, up_ref[...], preferred_element_type=jnp.float32)
        return jnp.square(jnp.maximum(wide, 0.0)).astype(jnp.bfloat16)

    first = hidden(theirs_ref[...])
    act_ref[...] = hidden(mine_ref[...])
    out_ref[...] = lax.dot_general(
        first, down_ref[...], (((1,), (1,)), ((), ())), preferred_element_type=jnp.float32
    ).astype(out_ref.dtype)


def mixer(at, theirs, mine, pieces):
    height, width = mine.shape
    units = pieces[0].shape[1] // 2
    smem = pl.BlockSpec(memory_space=pltpu.SMEM)
    vmem = pl.BlockSpec(memory_space=pltpu.VMEM)
    return pl.pallas_call(
        mixer_body,
        in_specs=[smem] + [vmem] * (2 + len(pieces)),
        out_specs=[vmem] * 3,
        out_shape=[
            jax.ShapeDtypeStruct((width, units), jnp.bfloat16),
            jax.ShapeDtypeStruct((height, units), jnp.bfloat16),
            jax.ShapeDtypeStruct((height, width), jnp.bfloat16),
        ],
        scratch_shapes=[pltpu.VMEM((width, units), jnp.bfloat16)],
        cost_estimate=pl.CostEstimate(flops=1 << 31, transcendentals=0, bytes_accessed=1 << 23),
        compiler_params=pltpu.CompilerParams(vmem_limit_bytes=40 << 20),
        name="mixer",
    )(at, theirs, mine, *pieces)


def attention_body(
    core_ref, slope_ref, sink_ref, q_ref, kt_ref, vt_ref, doc_ref, before_ref, after_ref,
    qg_ref, kg_ref, other_ref, own_ref, kn_ref, vn_ref, dk_ref
):
    head = kt_ref.shape[0]
    heads = q_ref.shape[1] // head
    kg = kg_ref[...]
    for j in range(6):
        if j == 0:
            kt, vt, doc = before_ref[:head, :], before_ref[head : 2 * head, :], before_ref[2 * head : 2 * head + 8, :]
        elif j == 5:
            kt, vt, doc = after_ref[:head, :], after_ref[head : 2 * head, :], after_ref[2 * head : 2 * head + 8, :]
        else:
            lanes = slice((j - 1) * WINDOW, j * WINDOW)
            kt, vt, doc = kt_ref[:, lanes], vt_ref[:, lanes], doc_ref[:8, lanes]
        wide = kt.astype(jnp.float32)
        scale = lax.rsqrt(jnp.mean(wide * wide, axis=0, keepdims=True) + EPS)
        kn_ref[j] = (wide * scale * kg).astype(jnp.bfloat16)
        vn_ref[j] = vt
        dk_ref[j] = doc.astype(jnp.float32)
    row = lax.broadcasted_iota(jnp.int32, (WINDOW, 3 * WINDOW), 0)
    col = lax.broadcasted_iota(jnp.int32, (WINDOW, 3 * WINDOW), 1)
    distance = jnp.abs(col - WINDOW - row)
    near = distance <= WINDOW
    far = distance.astype(jnp.float32)
    core = core_ref[0]
    for half in range(2):
        side = 1 - core if half == 0 else core
        for j in range(2):
            block = 2 * side + j
            q = q_ref[pl.ds(pl.multiple_of(block * WINDOW, WINDOW), WINDOW), :]
            keys = jnp.concatenate([kn_ref[block], kn_ref[block + 1], kn_ref[block + 2]], axis=1)
            vals = jnp.concatenate([vn_ref[block], vn_ref[block + 1], vn_ref[block + 2]], axis=1)
            doc_k = jnp.concatenate(
                [jnp.broadcast_to(dk_ref[block + i][:1], (WINDOW, WINDOW)) for i in range(3)], axis=1
            )
            doc_q = jnp.broadcast_to(dk_ref[block + 1][:1], (WINDOW, WINDOW)).T
            allowed = near & (doc_k == jnp.concatenate([doc_q] * 3, axis=1))
            outs = []
            for h in range(heads):
                wide = q[:, h * head : (h + 1) * head].astype(jnp.float32)
                scale = lax.rsqrt(jnp.mean(wide * wide, axis=-1, keepdims=True) + EPS)
                qn = (wide * scale * qg_ref[...]).astype(jnp.bfloat16)
                s = jnp.dot(qn, keys, preferred_element_type=jnp.float32) * head ** (-0.5)
                s = jnp.where(allowed, s - slope_ref[h] * far, jnp.float32(-1e30))
                top = jnp.maximum(jnp.max(s, axis=-1, keepdims=True), sink_ref[h])
                p = jnp.exp(s - top)
                denom = jnp.sum(p, axis=-1, keepdims=True) + jnp.exp(sink_ref[h] - top)
                mixed = lax.dot_general(
                    p.astype(jnp.bfloat16), vals, (((1,), (1,)), ((), ())),
                    preferred_element_type=jnp.float32,
                )
                outs.append((mixed / denom).astype(jnp.bfloat16))
            target = other_ref if half == 0 else own_ref
            target[j * WINDOW : (j + 1) * WINDOW, :] = jnp.concatenate(outs, axis=1)


def attention(core, slopes, sink, q, kt, vt, doc, before, after, q_gain, k_gain):
    head, rows = kt.shape
    smem = pl.BlockSpec(memory_space=pltpu.SMEM)
    vmem = pl.BlockSpec(memory_space=pltpu.VMEM)
    out = jax.ShapeDtypeStruct((rows // 2, q.shape[1]), jnp.bfloat16)
    return pl.pallas_call(
        attention_body,
        in_specs=[smem] * 3 + [vmem] * 8,
        out_specs=[vmem, vmem],
        out_shape=[out, out],
        scratch_shapes=[
            pltpu.VMEM((6, head, WINDOW), jnp.bfloat16),
            pltpu.VMEM((6, head, WINDOW), jnp.bfloat16),
            pltpu.VMEM((6, 8, WINDOW), jnp.float32),
        ],
        cost_estimate=pl.CostEstimate(flops=1 << 31, transcendentals=1 << 20, bytes_accessed=1 << 20),
        name="attend",
    )(core, slopes, sink, q, kt, vt, doc, before, after, q_gain, k_gain)


def shards(
    resid, queries, keys, values, documents, q_gain, k_gain, sink, w_out, n_gain, w_up, w_down
):
    rows = resid.shape[0]
    heads_here = sink.shape[0]
    core = lax.axis_index("c")
    half = rows // 2
    share = rows // lax.axis_size(TP)
    nx = lax.axis_size("x")

    kt, vt = keys.T, values.T
    doc = jnp.broadcast_to((documents + 1).astype(jnp.bfloat16)[None, :], (16, rows))
    packed = jnp.concatenate([kt, vt, doc], axis=0)
    count = lax.axis_size(SP)
    onward = [(i, i + 1) for i in range(count - 1)]
    before = lax.ppermute(packed[:, rows - WINDOW :], SP, onward)
    after = lax.ppermute(packed[:, :WINDOW], SP, [(j, i) for i, j in onward])
    piece = across(tie(jnp.concatenate([w_up, w_down.T], axis=1), packed))
    w_out_other = swap(w_out)

    heads_all = heads_here * lax.axis_size(TP)
    first_head = (lax.axis_index(TP) * heads_here).astype(jnp.float32)
    slopes = jnp.exp2(
        -8.0 * (first_head + jnp.arange(heads_here, dtype=jnp.float32) + 1.0) / heads_all
    )
    att_send, att_own = attention(
        core.astype(jnp.int32).reshape(1), slopes, sink, queries, kt, vt, doc, before, after,
        q_gain[None, :], k_gain[:, None],
    )
    piece = tie(piece, att_send)
    cut = piece.shape[0] // 2
    up1, dn1 = along(piece, 1), along(piece, -1)
    up2, dn2 = along(up1, 1), along(dn1, -1)
    up3, dn3 = along(up2, 1), along(dn2, -1)
    up4, dn4 = along(up3[:cut], 1), along(dn3[cut:], -1)
    pieces = [piece, dn1, dn2, dn3, up4, dn4, up3, up2, up1]

    att_other = swap(att_send)
    partial = jnp.dot(att_own, w_out, preferred_element_type=jnp.float32) + jnp.dot(
        att_other, w_out_other, preferred_element_type=jnp.float32
    )
    tiles = lax.all_to_all(
        partial.astype(jnp.bfloat16).reshape(nx, share, -1), "x", 0, 0, tiled=True
    )
    head_mix = jnp.sum(tiles.astype(jnp.float32), axis=0)
    start = core * half + lax.axis_index("x") * share
    own_resid = lax.dynamic_slice_in_dim(resid, start, share, 0)
    middle = (own_resid.astype(jnp.float32) + head_mix).astype(jnp.bfloat16)
    normed = rms_scale(middle, n_gain).astype(jnp.bfloat16)
    mine = spread(normed, "x")
    theirs = swap(mine)
    z, y = lax.axis_index("z"), lax.axis_index("y")
    chunk, block = w_up.shape[0], w_up.shape[0] * lax.axis_size("y")
    at = jnp.stack(
        [jnp.where(core == 0, y, z), jnp.where(core == 0, block, chunk), jnp.where(core == 0, chunk, block)]
    ).astype(jnp.int32)
    down_t, active, out = mixer(at, theirs, mine, pieces)
    sent = swap(out)
    kept = lax.optimization_barrier(
        lax.dot_general(
            active, down_t, (((1,), (1,)), ((), ())), preferred_element_type=jnp.float32
        )
    )
    joined = (kept + sent.astype(jnp.float32)).astype(jnp.bfloat16)
    unit_mix = scatter_x(joined)
    finished = spread((middle.astype(jnp.float32) + unit_mix).astype(jnp.bfloat16), "x")
    finished_other = swap(finished)
    low = jnp.where(core == 0, finished, finished_other)
    high = jnp.where(core == 0, finished_other, finished)
    return jnp.concatenate([low, high], axis=0)


def solution(mesh):
    fine = Mesh(mesh.devices.reshape(8, 8, 4, 2), ("z", "y", "x", "c"))
    placed = (
        P(SP, None),
        P(SP, TP),
        P(SP, TP),
        P(SP, TP),
        P(SP),
        P(),
        P(),
        P(TP),
        P(TP, None),
        P(),
        P(SP, TP),
        P(TP, SP),
    )
    return jax.shard_map(shards, mesh=fine, in_specs=placed, out_specs=P(SP, None), check_vma=False)
```

```python
import jax
import jax.numpy as jnp
from jax import lax
from jax.experimental import pallas as pl
from jax.experimental.pallas import tpu as pltpu
from jax.sharding import Mesh
from jax.sharding import PartitionSpec as P

WINDOW = 128
EPS = 1e-06
SP = ("z", "y")
TP = ("x", "c")


def along(x, by):
    nz, ny = lax.axis_size("z"), lax.axis_size("y")
    pairs = []
    for z in range(nz):
        for y in range(ny):
            here = 2 * (z * ny + y)
            pairs.append((here, 2 * (z * ny + (y + by) % ny)))
            pairs.append((here + 1, 2 * ((z + by) % nz * ny + y) + 1))
    return lax.ppermute(x, ("z", "y", "c"), pairs)


def across(copies):
    nz, ny = lax.axis_size("z"), lax.axis_size("y")
    groups = [[2 * (z * ny + y) for z in range(nz)] for y in range(ny)]
    groups += [[2 * (z * ny + y) + 1 for y in range(ny)] for z in range(nz)]
    tiles = lax.all_to_all(
        copies, ("z", "y", "c"), 0, 0, tiled=True, axis_index_groups=groups
    )
    return tiles.reshape(-1, tiles.shape[2])


def swap(x):
    return lax.ppermute(x, "c", [(0, 1), (1, 0)])


def spread(x, axis):
    n = lax.axis_size(axis)
    tiles = lax.all_to_all(jnp.broadcast_to(x, (n, *x.shape)), axis, 0, 0, tiled=True)
    return tiles.reshape(n * x.shape[0], x.shape[1])


def tie(x, y):
    return lax.optimization_barrier((x, y))[0]


def scatter_x(x):
    n = lax.axis_size("x")
    tiles = lax.all_to_all(x.reshape(n, x.shape[0] // n, x.shape[1]), "x", 0, 0, tiled=True)
    return jnp.sum(tiles.astype(jnp.float32), axis=0)


def rms_scale(field, gain):
    wide = field.astype(jnp.float32)
    return wide * lax.rsqrt(jnp.mean(wide * wide, axis=-1, keepdims=True) + EPS) * gain


def mixer_body(at_ref, theirs_ref, mine_ref, *refs):
    *pieces, down_ref, act_ref, out_ref, up_ref = refs
    count = len(pieces)
    units = act_ref.shape[1]
    chunk = pieces[0].shape[0] // count
    for r in range(count):
        index = lax.rem(at_ref[0] + r, count)
        for j in range(count):
            rows = slice(j * chunk, (j + 1) * chunk)
            to = pl.multiple_of(j * at_ref[1] + index * at_ref[2], chunk)
            up_ref[pl.ds(to, chunk), :] = pieces[r][rows, :units]
            down_ref[pl.ds(to, chunk), :] = pieces[r][rows, units:]

    def hidden(rows):
        wide = jnp.dot(rows, up_ref[...], preferred_element_type=jnp.float32)
        return jnp.square(jnp.maximum(wide, 0.0)).astype(jnp.bfloat16)

    first = hidden(theirs_ref[...])
    act_ref[...] = hidden(mine_ref[...])
    out_ref[...] = lax.dot_general(
        first, down_ref[...], (((1,), (1,)), ((), ())), preferred_element_type=jnp.float32
    ).astype(out_ref.dtype)


def mixer(at, theirs, mine, pieces):
    height, width = mine.shape
    units = pieces[0].shape[1] // 2
    smem = pl.BlockSpec(memory_space=pltpu.SMEM)
    vmem = pl.BlockSpec(memory_space=pltpu.VMEM)
    return pl.pallas_call(
        mixer_body,
        in_specs=[smem] + [vmem] * (2 + len(pieces)),
        out_specs=[vmem] * 3,
        out_shape=[
            jax.ShapeDtypeStruct((width, units), jnp.bfloat16),
            jax.ShapeDtypeStruct((height, units), jnp.bfloat16),
            jax.ShapeDtypeStruct((height, width), jnp.bfloat16),
        ],
        scratch_shapes=[pltpu.VMEM((width, units), jnp.bfloat16)],
        cost_estimate=pl.CostEstimate(flops=1 << 31, transcendentals=0, bytes_accessed=1 << 23),
        compiler_params=pltpu.CompilerParams(vmem_limit_bytes=40 << 20),
        name="mixer",
    )(at, theirs, mine, *pieces)


def attention_body(
    core_ref, slope_ref, sink_ref, q_ref, kt_ref, vt_ref, doc_ref, before_ref, after_ref,
    qg_ref, kg_ref, other_ref, own_ref, kn_ref, vn_ref, dk_ref
):
    head = kt_ref.shape[0]
    heads = q_ref.shape[1] // head
    kg = kg_ref[...]
    for j in range(6):
        if j == 0:
            kt, vt, doc = before_ref[:head, :], before_ref[head : 2 * head, :], before_ref[2 * head : 2 * head + 8, :]
        elif j == 5:
            kt, vt, doc = after_ref[:head, :], after_ref[head : 2 * head, :], after_ref[2 * head : 2 * head + 8, :]
        else:
            lanes = slice((j - 1) * WINDOW, j * WINDOW)
            kt, vt, doc = kt_ref[:, lanes], vt_ref[:, lanes], doc_ref[:8, lanes]
        wide = kt.astype(jnp.float32)
        scale = lax.rsqrt(jnp.mean(wide * wide, axis=0, keepdims=True) + EPS)
        kn_ref[j] = (wide * scale * kg).astype(jnp.bfloat16)
        vn_ref[j] = vt
        dk_ref[j] = doc.astype(jnp.float32)
    row = lax.broadcasted_iota(jnp.int32, (WINDOW, 3 * WINDOW), 0)
    col = lax.broadcasted_iota(jnp.int32, (WINDOW, 3 * WINDOW), 1)
    distance = jnp.abs(col - WINDOW - row)
    near = distance <= WINDOW
    far = distance.astype(jnp.float32)
    core = core_ref[0]
    for half in range(2):
        side = 1 - core if half == 0 else core
        for j in range(2):
            block = 2 * side + j
            q = q_ref[pl.ds(pl.multiple_of(block * WINDOW, WINDOW), WINDOW), :]
            keys = jnp.concatenate([kn_ref[block], kn_ref[block + 1], kn_ref[block + 2]], axis=1)
            vals = jnp.concatenate([vn_ref[block], vn_ref[block + 1], vn_ref[block + 2]], axis=1)
            doc_k = jnp.concatenate(
                [jnp.broadcast_to(dk_ref[block + i][:1], (WINDOW, WINDOW)) for i in range(3)], axis=1
            )
            doc_q = jnp.broadcast_to(dk_ref[block + 1][:1], (WINDOW, WINDOW)).T
            allowed = near & (doc_k == jnp.concatenate([doc_q] * 3, axis=1))
            outs = []
            for h in range(heads):
                wide = q[:, h * head : (h + 1) * head].astype(jnp.float32)
                scale = lax.rsqrt(jnp.mean(wide * wide, axis=-1, keepdims=True) + EPS)
                qn = (wide * scale * qg_ref[...]).astype(jnp.bfloat16)
                s = jnp.dot(qn, keys, preferred_element_type=jnp.float32) * head ** (-0.5)
                s = jnp.where(allowed, s - slope_ref[h] * far, jnp.float32(-1e30))
                top = jnp.maximum(jnp.max(s, axis=-1, keepdims=True), sink_ref[h])
                p = jnp.exp(s - top)
                denom = jnp.sum(p, axis=-1, keepdims=True) + jnp.exp(sink_ref[h] - top)
                mixed = lax.dot_general(
                    p.astype(jnp.bfloat16), vals, (((1,), (1,)), ((), ())),
                    preferred_element_type=jnp.float32,
                )
                outs.append((mixed / denom).astype(jnp.bfloat16))
            target = other_ref if half == 0 else own_ref
            target[j * WINDOW : (j + 1) * WINDOW, :] = jnp.concatenate(outs, axis=1)


def attention(core, slopes, sink, q, kt, vt, doc, before, after, q_gain, k_gain):
    head, rows = kt.shape
    smem = pl.BlockSpec(memory_space=pltpu.SMEM)
    vmem = pl.BlockSpec(memory_space=pltpu.VMEM)
    out = jax.ShapeDtypeStruct((rows // 2, q.shape[1]), jnp.bfloat16)
    return pl.pallas_call(
        attention_body,
        in_specs=[smem] * 3 + [vmem] * 8,
        out_specs=[vmem, vmem],
        out_shape=[out, out],
        scratch_shapes=[
            pltpu.VMEM((6, head, WINDOW), jnp.bfloat16),
            pltpu.VMEM((6, head, WINDOW), jnp.bfloat16),
            pltpu.VMEM((6, 8, WINDOW), jnp.float32),
        ],
        cost_estimate=pl.CostEstimate(flops=1 << 31, transcendentals=1 << 20, bytes_accessed=1 << 20),
        name="attend",
    )(core, slopes, sink, q, kt, vt, doc, before, after, q_gain, k_gain)


def shards(
    resid, queries, keys, values, documents, q_gain, k_gain, sink, w_out, n_gain, w_up, w_down
):
    rows = resid.shape[0]
    heads_here = sink.shape[0]
    core = lax.axis_index("c")
    half = rows // 2
    share = rows // lax.axis_size(TP)
    nx = lax.axis_size("x")

    kt, vt = keys.T, values.T
    doc = jnp.broadcast_to((documents + 1).astype(jnp.bfloat16)[None, :], (16, rows))
    packed = jnp.concatenate([kt, vt, doc], axis=0)
    count = lax.axis_size(SP)
    onward = [(i, i + 1) for i in range(count - 1)]
    before = lax.ppermute(packed[:, rows - WINDOW :], SP, onward)
    after = lax.ppermute(packed[:, :WINDOW], SP, [(j, i) for i, j in onward])
    both = tie(jnp.concatenate([w_up, w_down.T], axis=1), packed)
    piece = across(jnp.broadcast_to(both, (lax.axis_size("z"), *both.shape)))
    w_out_other = swap(w_out)

    heads_all = heads_here * lax.axis_size(TP)
    first_head = (lax.axis_index(TP) * heads_here).astype(jnp.float32)
    slopes = jnp.exp2(
        -8.0 * (first_head + jnp.arange(heads_here, dtype=jnp.float32) + 1.0) / heads_all
    )
    att_send, att_own = attention(
        core.astype(jnp.int32).reshape(1), slopes, sink, queries, kt, vt, doc, before, after,
        q_gain[None, :], k_gain[:, None],
    )
    piece = tie(piece, att_send)
    up1, dn1 = along(piece, 1), along(piece, -1)
    up2, dn2 = along(up1, 1), along(dn1, -1)
    up3, dn3 = along(up2, 1), along(dn2, -1)
    up4 = along(up3, 1)
    pieces = [piece, dn1, dn2, dn3, up4, up3, up2, up1]

    att_other = swap(att_send)
    partial = jnp.dot(att_own, w_out, preferred_element_type=jnp.float32) + jnp.dot(
        att_other, w_out_other, preferred_element_type=jnp.float32
    )
    tiles = lax.all_to_all(
        partial.astype(jnp.bfloat16).reshape(nx, share, -1), "x", 0, 0, tiled=True
    )
    head_mix = jnp.sum(tiles.astype(jnp.float32), axis=0)
    start = core * half + lax.axis_index("x") * share
    own_resid = lax.dynamic_slice_in_dim(resid, start, share, 0)
    middle = (own_resid.astype(jnp.float32) + head_mix).astype(jnp.bfloat16)
    normed = rms_scale(middle, n_gain).astype(jnp.bfloat16)
    mine = spread(normed, "x")
    theirs = swap(mine)
    z, y = lax.axis_index("z"), lax.axis_index("y")
    chunk, block = w_up.shape[0], w_up.shape[0] * lax.axis_size("y")
    at = jnp.stack(
        [jnp.where(core == 0, y, z), jnp.where(core == 0, block, chunk), jnp.where(core == 0, chunk, block)]
    ).astype(jnp.int32)
    down_t, active, out = mixer(at, theirs, mine, pieces)
    sent = swap(out)
    kept = lax.optimization_barrier(
        lax.dot_general(
            active, down_t, (((1,), (1,)), ((), ())), preferred_element_type=jnp.float32
        )
    )
    joined = (kept + sent.astype(jnp.float32)).astype(jnp.bfloat16)
    unit_mix = scatter_x(joined)
    finished = spread((middle.astype(jnp.float32) + unit_mix).astype(jnp.bfloat16), "x")
    finished_other = swap(finished)
    out = lax.dynamic_update_slice_in_dim(
        jnp.zeros(resid.shape, resid.dtype), finished, core * half, 0
    )
    out = lax.optimization_barrier(out)
    return lax.dynamic_update_slice_in_dim(out, finished_other, (1 - core) * half, 0)


def solution(mesh):
    fine = Mesh(mesh.devices.reshape(8, 8, 4, 2), ("z", "y", "x", "c"))
    placed = (
        P(SP, None),
        P(SP, TP),
        P(SP, TP),
        P(SP, TP),
        P(SP),
        P(),
        P(),
        P(TP),
        P(TP, None),
        P(),
        P(SP, TP),
        P(TP, SP),
    )
    return jax.shard_map(shards, mesh=fine, in_specs=placed, out_specs=P(SP, None), check_vma=False)
```

```python
import jax
import jax.numpy as jnp
from jax import lax
from jax.experimental import pallas as pl
from jax.experimental.pallas import tpu as pltpu
from jax.sharding import Mesh
from jax.sharding import PartitionSpec as P

WINDOW = 128
EPS = 1e-06
SP = ("z", "y")
TP = ("x", "c")


def along(x, by):
    nz, ny = lax.axis_size("z"), lax.axis_size("y")
    pairs = []
    for z in range(nz):
        for y in range(ny):
            here = 2 * (z * ny + y)
            pairs.append((here, 2 * (z * ny + (y + by) % ny)))
            pairs.append((here + 1, 2 * ((z + by) % nz * ny + y) + 1))
    return lax.ppermute(x, ("z", "y", "c"), pairs)


def across(copies):
    nz, ny = lax.axis_size("z"), lax.axis_size("y")
    groups = [[2 * (z * ny + y) for z in range(nz)] for y in range(ny)]
    groups += [[2 * (z * ny + y) + 1 for y in range(ny)] for z in range(nz)]
    tiles = lax.all_to_all(
        copies, ("z", "y", "c"), 0, 0, tiled=True, axis_index_groups=groups
    )
    return tiles.reshape(-1, tiles.shape[2])


def swap(x):
    return lax.ppermute(x, "c", [(0, 1), (1, 0)])


def spread(x, axis):
    n = lax.axis_size(axis)
    tiles = lax.all_to_all(jnp.broadcast_to(x, (n, *x.shape)), axis, 0, 0, tiled=True)
    return tiles.reshape(n * x.shape[0], x.shape[1])


def scatter_x(x):
    n = lax.axis_size("x")
    tiles = lax.all_to_all(x.reshape(n, x.shape[0] // n, x.shape[1]), "x", 0, 0, tiled=True)
    return jnp.sum(tiles.astype(jnp.float32), axis=0)


def rms_scale(field, gain):
    wide = field.astype(jnp.float32)
    return wide * lax.rsqrt(jnp.mean(wide * wide, axis=-1, keepdims=True) + EPS) * gain


def mixer_body(at_ref, theirs_ref, mine_ref, *refs):
    *pieces, down_ref, act_ref, out_ref, up_ref = refs
    count = len(pieces) - 1
    units = act_ref.shape[1]
    cut = pieces[count // 2].shape[0]
    chunk = 2 * cut // count
    for r in range(count):
        index = lax.rem(at_ref[0] + r, count)
        for j in range(count):
            if r < count // 2:
                source, low = pieces[r], j * chunk
            elif r > count // 2:
                source, low = pieces[r + 1], j * chunk
            else:
                source, low = pieces[r + j * chunk // cut], j * chunk % cut
            to = pl.multiple_of(j * at_ref[1] + index * at_ref[2], chunk)
            up_ref[pl.ds(to, chunk), :] = source[low : low + chunk, :units]
            down_ref[pl.ds(to, chunk), :] = source[low : low + chunk, units:]

    def hidden(rows):
        wide = jnp.dot(rows, up_ref[...], preferred_element_type=jnp.float32)
        return jnp.square(jnp.maximum(wide, 0.0)).astype(jnp.bfloat16)

    first = hidden(theirs_ref[...])
    act_ref[...] = hidden(mine_ref[...])
    out_ref[...] = lax.dot_general(
        first, down_ref[...], (((1,), (1,)), ((), ())), preferred_element_type=jnp.float32
    ).astype(out_ref.dtype)


def mixer(at, theirs, mine, pieces):
    height, width = mine.shape
    units = pieces[0].shape[1] // 2
    smem = pl.BlockSpec(memory_space=pltpu.SMEM)
    vmem = pl.BlockSpec(memory_space=pltpu.VMEM)
    return pl.pallas_call(
        mixer_body,
        in_specs=[smem] + [vmem] * (2 + len(pieces)),
        out_specs=[vmem] * 3,
        out_shape=[
            jax.ShapeDtypeStruct((width, units), jnp.bfloat16),
            jax.ShapeDtypeStruct((height, units), jnp.bfloat16),
            jax.ShapeDtypeStruct((height, width), jnp.bfloat16),
        ],
        scratch_shapes=[pltpu.VMEM((width, units), jnp.bfloat16)],
        cost_estimate=pl.CostEstimate(flops=1 << 31, transcendentals=0, bytes_accessed=1 << 23),
        compiler_params=pltpu.CompilerParams(vmem_limit_bytes=40 << 20),
        name="mixer",
    )(at, theirs, mine, *pieces)


def attention_body(
    core_ref, slope_ref, sink_ref, q_ref, kt_ref, vt_ref, doc_ref, before_ref, after_ref,
    qg_ref, kg_ref, other_ref, own_ref, kn_ref, vn_ref, dk_ref
):
    head = kt_ref.shape[0]
    heads = q_ref.shape[1] // head
    kg = kg_ref[...]
    for j in range(6):
        if j == 0:
            kt, vt, doc = before_ref[:head, :], before_ref[head : 2 * head, :], before_ref[2 * head : 2 * head + 8, :]
        elif j == 5:
            kt, vt, doc = after_ref[:head, :], after_ref[head : 2 * head, :], after_ref[2 * head : 2 * head + 8, :]
        else:
            lanes = slice((j - 1) * WINDOW, j * WINDOW)
            kt, vt, doc = kt_ref[:, lanes], vt_ref[:, lanes], doc_ref[:8, lanes]
        wide = kt.astype(jnp.float32)
        scale = lax.rsqrt(jnp.mean(wide * wide, axis=0, keepdims=True) + EPS)
        kn_ref[j] = (wide * scale * kg).astype(jnp.bfloat16)
        vn_ref[j] = vt
        dk_ref[j] = doc.astype(jnp.float32)
    row = lax.broadcasted_iota(jnp.int32, (WINDOW, 3 * WINDOW), 0)
    col = lax.broadcasted_iota(jnp.int32, (WINDOW, 3 * WINDOW), 1)
    distance = jnp.abs(col - WINDOW - row)
    near = distance <= WINDOW
    far = distance.astype(jnp.float32)
    core = core_ref[0]
    for half in range(2):
        side = 1 - core if half == 0 else core
        for j in range(2):
            block = 2 * side + j
            q = q_ref[pl.ds(pl.multiple_of(block * WINDOW, WINDOW), WINDOW), :]
            keys = jnp.concatenate([kn_ref[block], kn_ref[block + 1], kn_ref[block + 2]], axis=1)
            vals = jnp.concatenate([vn_ref[block], vn_ref[block + 1], vn_ref[block + 2]], axis=1)
            doc_k = jnp.concatenate(
                [jnp.broadcast_to(dk_ref[block + i][:1], (WINDOW, WINDOW)) for i in range(3)], axis=1
            )
            doc_q = jnp.broadcast_to(dk_ref[block + 1][:1], (WINDOW, WINDOW)).T
            allowed = near & (doc_k == jnp.concatenate([doc_q] * 3, axis=1))
            outs = []
            for h in range(heads):
                wide = q[:, h * head : (h + 1) * head].astype(jnp.float32)
                scale = lax.rsqrt(jnp.mean(wide * wide, axis=-1, keepdims=True) + EPS)
                qn = (wide * scale * qg_ref[...]).astype(jnp.bfloat16)
                s = jnp.dot(qn, keys, preferred_element_type=jnp.float32) * head ** (-0.5)
                s = jnp.where(allowed, s - slope_ref[h] * far, jnp.float32(-1e30))
                top = jnp.maximum(jnp.max(s, axis=-1, keepdims=True), sink_ref[h])
                p = jnp.exp(s - top)
                denom = jnp.sum(p, axis=-1, keepdims=True) + jnp.exp(sink_ref[h] - top)
                mixed = lax.dot_general(
                    p.astype(jnp.bfloat16), vals, (((1,), (1,)), ((), ())),
                    preferred_element_type=jnp.float32,
                )
                outs.append((mixed / denom).astype(jnp.bfloat16))
            target = other_ref if half == 0 else own_ref
            target[j * WINDOW : (j + 1) * WINDOW, :] = jnp.concatenate(outs, axis=1)


def attention(core, slopes, sink, q, kt, vt, doc, before, after, q_gain, k_gain):
    head, rows = kt.shape
    smem = pl.BlockSpec(memory_space=pltpu.SMEM)
    vmem = pl.BlockSpec(memory_space=pltpu.VMEM)
    out = jax.ShapeDtypeStruct((rows // 2, q.shape[1]), jnp.bfloat16)
    return pl.pallas_call(
        attention_body,
        in_specs=[smem] * 3 + [vmem] * 8,
        out_specs=[vmem, vmem],
        out_shape=[out, out],
        scratch_shapes=[
            pltpu.VMEM((6, head, WINDOW), jnp.bfloat16),
            pltpu.VMEM((6, head, WINDOW), jnp.bfloat16),
            pltpu.VMEM((6, 8, WINDOW), jnp.float32),
        ],
        cost_estimate=pl.CostEstimate(flops=1 << 31, transcendentals=1 << 20, bytes_accessed=1 << 20),
        name="attend",
    )(core, slopes, sink, q, kt, vt, doc, before, after, q_gain, k_gain)


def shards(
    resid, queries, keys, values, documents, q_gain, k_gain, sink, w_out, n_gain, w_up, w_down
):
    rows = resid.shape[0]
    heads_here = sink.shape[0]
    core = lax.axis_index("c")
    half = rows // 2
    share = rows // lax.axis_size(TP)
    nx = lax.axis_size("x")

    kt, vt = keys.T, values.T
    doc = jnp.broadcast_to((documents + 1).astype(jnp.bfloat16)[None, :], (16, rows))
    packed = jnp.concatenate([kt, vt, doc], axis=0)
    count = lax.axis_size(SP)
    onward = [(i, i + 1) for i in range(count - 1)]
    before = lax.ppermute(packed[:, rows - WINDOW :], SP, onward)
    after = lax.ppermute(packed[:, :WINDOW], SP, [(j, i) for i, j in onward])
    both = jnp.concatenate([w_up, w_down.T], axis=1)
    piece = across(jnp.broadcast_to(both, (lax.axis_size("z"), *both.shape)))
    w_out_other = swap(w_out)

    heads_all = heads_here * lax.axis_size(TP)
    first_head = (lax.axis_index(TP) * heads_here).astype(jnp.float32)
    slopes = jnp.exp2(
        -8.0 * (first_head + jnp.arange(heads_here, dtype=jnp.float32) + 1.0) / heads_all
    )
    att_send, att_own = attention(
        core.astype(jnp.int32).reshape(1), slopes, sink, queries, kt, vt, doc, before, after,
        q_gain[None, :], k_gain[:, None],
    )
    cut = piece.shape[0] // 2
    up1, dn1 = along(piece, 1), along(piece, -1)
    up2, dn2 = along(up1, 1), along(dn1, -1)
    up3, dn3 = along(up2, 1), along(dn2, -1)
    up4, dn4 = along(up3[:cut], 1), along(dn3[cut:], -1)
    pieces = [piece, dn1, dn2, dn3, up4, dn4, up3, up2, up1]

    att_other = swap(att_send)
    partial = jnp.dot(att_own, w_out, preferred_element_type=jnp.float32) + jnp.dot(
        att_other, w_out_other, preferred_element_type=jnp.float32
    )
    tiles = lax.all_to_all(
        partial.astype(jnp.bfloat16).reshape(nx, share, -1), "x", 0, 0, tiled=True
    )
    head_mix = jnp.sum(tiles.astype(jnp.float32), axis=0)
    start = core * half + lax.axis_index("x") * share
    own_resid = lax.dynamic_slice_in_dim(resid, start, share, 0)
    middle = (own_resid.astype(jnp.float32) + head_mix).astype(jnp.bfloat16)
    normed = rms_scale(middle, n_gain).astype(jnp.bfloat16)
    mine = spread(normed, "x")
    theirs = swap(mine)
    z, y = lax.axis_index("z"), lax.axis_index("y")
    chunk, block = w_up.shape[0], w_up.shape[0] * lax.axis_size("y")
    at = jnp.stack(
        [jnp.where(core == 0, y, z), jnp.where(core == 0, block, chunk), jnp.where(core == 0, chunk, block)]
    ).astype(jnp.int32)
    down_t, active, out = mixer(at, theirs, mine, pieces)
    sent = swap(out)
    kept = lax.optimization_barrier(
        lax.dot_general(
            active, down_t, (((1,), (1,)), ((), ())), preferred_element_type=jnp.float32
        )
    )
    joined = (kept + sent.astype(jnp.float32)).astype(jnp.bfloat16)
    unit_mix = scatter_x(joined)
    finished = spread((middle.astype(jnp.float32) + unit_mix).astype(jnp.bfloat16), "x")
    finished_other = swap(finished)
    out = lax.dynamic_update_slice_in_dim(
        jnp.zeros(resid.shape, resid.dtype), finished, core * half, 0
    )
    out = lax.optimization_barrier(out)
    return lax.dynamic_update_slice_in_dim(out, finished_other, (1 - core) * half, 0)


def solution(mesh):
    fine = Mesh(mesh.devices.reshape(8, 8, 4, 2), ("z", "y", "x", "c"))
    placed = (
        P(SP, None),
        P(SP, TP),
        P(SP, TP),
        P(SP, TP),
        P(SP),
        P(),
        P(),
        P(TP),
        P(TP, None),
        P(),
        P(SP, TP),
        P(TP, SP),
    )
    return jax.shard_map(shards, mesh=fine, in_specs=placed, out_specs=P(SP, None), check_vma=False)
```

```python
import jax
import jax.numpy as jnp
from jax import lax
from jax.experimental import pallas as pl
from jax.experimental.pallas import tpu as pltpu
from jax.sharding import Mesh
from jax.sharding import PartitionSpec as P

WINDOW = 128
EPS = 1e-06
SP = ("z", "y")
TP = ("x", "c")


def along(x, by):
    nz, ny = lax.axis_size("z"), lax.axis_size("y")
    pairs = []
    for z in range(nz):
        for y in range(ny):
            here = 2 * (z * ny + y)
            pairs.append((here, 2 * (z * ny + (y + by) % ny)))
            pairs.append((here + 1, 2 * ((z + by) % nz * ny + y) + 1))
    return lax.ppermute(x, ("z", "y", "c"), pairs)


def across(copies):
    nz, ny = lax.axis_size("z"), lax.axis_size("y")
    groups = [[2 * (z * ny + y) for z in range(nz)] for y in range(ny)]
    groups += [[2 * (z * ny + y) + 1 for y in range(ny)] for z in range(nz)]
    tiles = lax.all_to_all(
        copies, ("z", "y", "c"), 0, 0, tiled=True, axis_index_groups=groups
    )
    return tiles.reshape(-1, tiles.shape[2])


def swap(x):
    return lax.ppermute(x, "c", [(0, 1), (1, 0)])


def spread(x, axis):
    n = lax.axis_size(axis)
    tiles = lax.all_to_all(jnp.broadcast_to(x, (n, *x.shape)), axis, 0, 0, tiled=True)
    return tiles.reshape(n * x.shape[0], x.shape[1])


def copies_body(up_ref, down_ref, out_ref):
    units = up_ref.shape[1]
    for i in range(out_ref.shape[0]):
        out_ref[i, :, :units] = up_ref[...]
        out_ref[i, :, units:] = down_ref[...]


def copies_of(up, down_t, count):
    rows, units = up.shape
    vmem = pl.BlockSpec(memory_space=pltpu.VMEM)
    return pl.pallas_call(
        copies_body,
        in_specs=[vmem, vmem],
        out_specs=vmem,
        out_shape=jax.ShapeDtypeStruct((count, rows, 2 * units), up.dtype),
        name="copies",
    )(up, down_t)


def scatter_x(x):
    n = lax.axis_size("x")
    tiles = lax.all_to_all(x.reshape(n, x.shape[0] // n, x.shape[1]), "x", 0, 0, tiled=True)
    return jnp.sum(tiles.astype(jnp.float32), axis=0)


def rms_scale(field, gain):
    wide = field.astype(jnp.float32)
    return wide * lax.rsqrt(jnp.mean(wide * wide, axis=-1, keepdims=True) + EPS) * gain


def mixer_body(at_ref, theirs_ref, mine_ref, *refs):
    *pieces, down_ref, act_ref, out_ref, up_ref = refs
    count = len(pieces) - 1
    units = act_ref.shape[1]
    cut = pieces[count // 2].shape[0]
    chunk = 2 * cut // count
    for r in range(count):
        index = lax.rem(at_ref[0] + r, count)
        for j in range(count):
            if r < count // 2:
                source, low = pieces[r], j * chunk
            elif r > count // 2:
                source, low = pieces[r + 1], j * chunk
            else:
                source, low = pieces[r + j * chunk // cut], j * chunk % cut
            to = pl.multiple_of(j * at_ref[1] + index * at_ref[2], chunk)
            up_ref[pl.ds(to, chunk), :] = source[low : low + chunk, :units]
            down_ref[pl.ds(to, chunk), :] = source[low : low + chunk, units:]

    def hidden(rows):
        wide = jnp.dot(rows, up_ref[...], preferred_element_type=jnp.float32)
        return jnp.square(jnp.maximum(wide, 0.0)).astype(jnp.bfloat16)

    first = hidden(theirs_ref[...])
    act_ref[...] = hidden(mine_ref[...])
    out_ref[...] = lax.dot_general(
        first, down_ref[...], (((1,), (1,)), ((), ())), preferred_element_type=jnp.float32
    ).astype(out_ref.dtype)


def mixer(at, theirs, mine, pieces):
    height, width = mine.shape
    units = pieces[0].shape[1] // 2
    smem = pl.BlockSpec(memory_space=pltpu.SMEM)
    vmem = pl.BlockSpec(memory_space=pltpu.VMEM)
    return pl.pallas_call(
        mixer_body,
        in_specs=[smem] + [vmem] * (2 + len(pieces)),
        out_specs=[vmem] * 3,
        out_shape=[
            jax.ShapeDtypeStruct((width, units), jnp.bfloat16),
            jax.ShapeDtypeStruct((height, units), jnp.bfloat16),
            jax.ShapeDtypeStruct((height, width), jnp.bfloat16),
        ],
        scratch_shapes=[pltpu.VMEM((width, units), jnp.bfloat16)],
        cost_estimate=pl.CostEstimate(flops=1 << 31, transcendentals=0, bytes_accessed=1 << 23),
        compiler_params=pltpu.CompilerParams(vmem_limit_bytes=40 << 20),
        name="mixer",
    )(at, theirs, mine, *pieces)


def attention_body(
    core_ref, slope_ref, sink_ref, q_ref, kt_ref, vt_ref, doc_ref, before_ref, after_ref,
    qg_ref, kg_ref, other_ref, own_ref, kn_ref, vn_ref, dk_ref
):
    head = kt_ref.shape[0]
    heads = q_ref.shape[1] // head
    kg = kg_ref[...]
    for j in range(6):
        if j == 0:
            kt, vt, doc = before_ref[:head, :], before_ref[head : 2 * head, :], before_ref[2 * head : 2 * head + 8, :]
        elif j == 5:
            kt, vt, doc = after_ref[:head, :], after_ref[head : 2 * head, :], after_ref[2 * head : 2 * head + 8, :]
        else:
            lanes = slice((j - 1) * WINDOW, j * WINDOW)
            kt, vt, doc = kt_ref[:, lanes], vt_ref[:, lanes], doc_ref[:8, lanes]
        wide = kt.astype(jnp.float32)
        scale = lax.rsqrt(jnp.mean(wide * wide, axis=0, keepdims=True) + EPS)
        kn_ref[j] = (wide * scale * kg).astype(jnp.bfloat16)
        vn_ref[j] = vt
        dk_ref[j] = doc.astype(jnp.float32)
    row = lax.broadcasted_iota(jnp.int32, (WINDOW, 3 * WINDOW), 0)
    col = lax.broadcasted_iota(jnp.int32, (WINDOW, 3 * WINDOW), 1)
    distance = jnp.abs(col - WINDOW - row)
    near = distance <= WINDOW
    far = distance.astype(jnp.float32)
    core = core_ref[0]
    for half in range(2):
        side = 1 - core if half == 0 else core
        for j in range(2):
            block = 2 * side + j
            q = q_ref[pl.ds(pl.multiple_of(block * WINDOW, WINDOW), WINDOW), :]
            keys = jnp.concatenate([kn_ref[block], kn_ref[block + 1], kn_ref[block + 2]], axis=1)
            vals = jnp.concatenate([vn_ref[block], vn_ref[block + 1], vn_ref[block + 2]], axis=1)
            doc_k = jnp.concatenate(
                [jnp.broadcast_to(dk_ref[block + i][:1], (WINDOW, WINDOW)) for i in range(3)], axis=1
            )
            doc_q = jnp.broadcast_to(dk_ref[block + 1][:1], (WINDOW, WINDOW)).T
            allowed = near & (doc_k == jnp.concatenate([doc_q] * 3, axis=1))
            outs = []
            for h in range(heads):
                wide = q[:, h * head : (h + 1) * head].astype(jnp.float32)
                scale = lax.rsqrt(jnp.mean(wide * wide, axis=-1, keepdims=True) + EPS)
                qn = (wide * scale * qg_ref[...]).astype(jnp.bfloat16)
                s = jnp.dot(qn, keys, preferred_element_type=jnp.float32) * head ** (-0.5)
                s = jnp.where(allowed, s - slope_ref[h] * far, jnp.float32(-1e30))
                top = jnp.maximum(jnp.max(s, axis=-1, keepdims=True), sink_ref[h])
                p = jnp.exp(s - top)
                denom = jnp.sum(p, axis=-1, keepdims=True) + jnp.exp(sink_ref[h] - top)
                mixed = lax.dot_general(
                    p.astype(jnp.bfloat16), vals, (((1,), (1,)), ((), ())),
                    preferred_element_type=jnp.float32,
                )
                outs.append((mixed / denom).astype(jnp.bfloat16))
            target = other_ref if half == 0 else own_ref
            target[j * WINDOW : (j + 1) * WINDOW, :] = jnp.concatenate(outs, axis=1)


def attention(core, slopes, sink, q, kt, vt, doc, before, after, q_gain, k_gain):
    head, rows = kt.shape
    smem = pl.BlockSpec(memory_space=pltpu.SMEM)
    vmem = pl.BlockSpec(memory_space=pltpu.VMEM)
    out = jax.ShapeDtypeStruct((rows // 2, q.shape[1]), jnp.bfloat16)
    return pl.pallas_call(
        attention_body,
        in_specs=[smem] * 3 + [vmem] * 8,
        out_specs=[vmem, vmem],
        out_shape=[out, out],
        scratch_shapes=[
            pltpu.VMEM((6, head, WINDOW), jnp.bfloat16),
            pltpu.VMEM((6, head, WINDOW), jnp.bfloat16),
            pltpu.VMEM((6, 8, WINDOW), jnp.float32),
        ],
        cost_estimate=pl.CostEstimate(flops=1 << 31, transcendentals=1 << 20, bytes_accessed=1 << 20),
        name="attend",
    )(core, slopes, sink, q, kt, vt, doc, before, after, q_gain, k_gain)


def shards(
    resid, queries, keys, values, documents, q_gain, k_gain, sink, w_out, n_gain, w_up, w_down
):
    rows = resid.shape[0]
    heads_here = sink.shape[0]
    core = lax.axis_index("c")
    half = rows // 2
    share = rows // lax.axis_size(TP)
    nx = lax.axis_size("x")

    kt, vt = keys.T, values.T
    doc = jnp.broadcast_to((documents + 1).astype(jnp.bfloat16)[None, :], (16, rows))
    packed = jnp.concatenate([kt, vt, doc], axis=0)
    count = lax.axis_size(SP)
    onward = [(i, i + 1) for i in range(count - 1)]
    before = lax.ppermute(packed[:, rows - WINDOW :], SP, onward)
    after = lax.ppermute(packed[:, :WINDOW], SP, [(j, i) for i, j in onward])
    piece = across(copies_of(w_up, w_down.T, lax.axis_size("z")))
    w_out_other = swap(w_out)

    heads_all = heads_here * lax.axis_size(TP)
    first_head = (lax.axis_index(TP) * heads_here).astype(jnp.float32)
    slopes = jnp.exp2(
        -8.0 * (first_head + jnp.arange(heads_here, dtype=jnp.float32) + 1.0) / heads_all
    )
    att_send, att_own = attention(
        core.astype(jnp.int32).reshape(1), slopes, sink, queries, kt, vt, doc, before, after,
        q_gain[None, :], k_gain[:, None],
    )
    cut = piece.shape[0] // 2
    up1, dn1 = along(piece, 1), along(piece, -1)
    up2, dn2 = along(up1, 1), along(dn1, -1)
    up3, dn3 = along(up2, 1), along(dn2, -1)
    up4, dn4 = along(up2[:cut], 2), along(dn2[cut:], -2)
    pieces = [piece, dn1, dn2, dn3, up4, dn4, up3, up2, up1]

    att_other = swap(att_send)
    partial = jnp.dot(att_own, w_out, preferred_element_type=jnp.float32) + jnp.dot(
        att_other, w_out_other, preferred_element_type=jnp.float32
    )
    tiles = lax.all_to_all(
        partial.astype(jnp.bfloat16).reshape(nx, share, -1), "x", 0, 0, tiled=True
    )
    head_mix = jnp.sum(tiles.astype(jnp.float32), axis=0)
    start = core * half + lax.axis_index("x") * share
    own_resid = lax.dynamic_slice_in_dim(resid, start, share, 0)
    middle = (own_resid.astype(jnp.float32) + head_mix).astype(jnp.bfloat16)
    normed = rms_scale(middle, n_gain).astype(jnp.bfloat16)
    mine = spread(normed, "x")
    theirs = swap(mine)
    z, y = lax.axis_index("z"), lax.axis_index("y")
    chunk, block = w_up.shape[0], w_up.shape[0] * lax.axis_size("y")
    at = jnp.stack(
        [jnp.where(core == 0, y, z), jnp.where(core == 0, block, chunk), jnp.where(core == 0, chunk, block)]
    ).astype(jnp.int32)
    down_t, active, out = mixer(at, theirs, mine, pieces)
    sent = swap(out)
    kept = lax.optimization_barrier(
        lax.dot_general(
            active, down_t, (((1,), (1,)), ((), ())), preferred_element_type=jnp.float32
        )
    )
    joined = (kept + sent.astype(jnp.float32)).astype(jnp.bfloat16)
    unit_mix = scatter_x(joined)
    finished = spread((middle.astype(jnp.float32) + unit_mix).astype(jnp.bfloat16), "x")
    finished_other = swap(finished)
    out = lax.dynamic_update_slice_in_dim(
        jnp.zeros(resid.shape, resid.dtype), finished, core * half, 0
    )
    out = lax.optimization_barrier(out)
    return lax.dynamic_update_slice_in_dim(out, finished_other, (1 - core) * half, 0)


def solution(mesh):
    fine = Mesh(mesh.devices.reshape(8, 8, 4, 2), ("z", "y", "x", "c"))
    placed = (
        P(SP, None),
        P(SP, TP),
        P(SP, TP),
        P(SP, TP),
        P(SP),
        P(),
        P(),
        P(TP),
        P(TP, None),
        P(),
        P(SP, TP),
        P(TP, SP),
    )
    return jax.shard_map(shards, mesh=fine, in_specs=placed, out_specs=P(SP, None), check_vma=False)
```

```python
import jax
import jax.numpy as jnp
from jax import lax
from jax.experimental import pallas as pl
from jax.experimental.pallas import tpu as pltpu
from jax.sharding import Mesh
from jax.sharding import PartitionSpec as P

WINDOW = 128
EPS = 1e-06
SP = ("z", "y")
TP = ("x", "c")


def along(x, by):
    nz, ny = lax.axis_size("z"), lax.axis_size("y")
    pairs = []
    for z in range(nz):
        for y in range(ny):
            here = 2 * (z * ny + y)
            pairs.append((here, 2 * (z * ny + (y + by) % ny)))
            pairs.append((here + 1, 2 * ((z + by) % nz * ny + y) + 1))
    return lax.ppermute(x, ("z", "y", "c"), pairs)


def across(copies):
    nz, ny = lax.axis_size("z"), lax.axis_size("y")
    groups = [[2 * (z * ny + y) for z in range(nz)] for y in range(ny)]
    groups += [[2 * (z * ny + y) + 1 for y in range(ny)] for z in range(nz)]
    tiles = lax.all_to_all(
        copies, ("z", "y", "c"), 0, 0, tiled=True, axis_index_groups=groups
    )
    return tiles.reshape(-1, tiles.shape[2])


def swap(x):
    return lax.ppermute(x, "c", [(0, 1), (1, 0)])


def spread(x, axis):
    n = lax.axis_size(axis)
    tiles = lax.all_to_all(jnp.broadcast_to(x, (n, *x.shape)), axis, 0, 0, tiled=True)
    return tiles.reshape(n * x.shape[0], x.shape[1])


def copies_body(up_ref, down_ref, out_ref):
    units = up_ref.shape[1]
    for i in range(out_ref.shape[0]):
        out_ref[i, :, :units] = up_ref[...]
        out_ref[i, :, units:] = down_ref[...]


def copies_of(up, down_t, count):
    rows, units = up.shape
    vmem = pl.BlockSpec(memory_space=pltpu.VMEM)
    return pl.pallas_call(
        copies_body,
        in_specs=[vmem, vmem],
        out_specs=vmem,
        out_shape=pltpu.VMEM((count, rows, 2 * units), up.dtype),
        name="copies",
    )(up, down_t)


def scatter_x(x):
    n = lax.axis_size("x")
    tiles = lax.all_to_all(x.reshape(n, x.shape[0] // n, x.shape[1]), "x", 0, 0, tiled=True)
    return jnp.sum(tiles.astype(jnp.float32), axis=0)


def rms_scale(field, gain):
    wide = field.astype(jnp.float32)
    return wide * lax.rsqrt(jnp.mean(wide * wide, axis=-1, keepdims=True) + EPS) * gain


def place(at_ref, r, count, chunk, source, put):
    index = lax.rem(at_ref[0] + r, count)
    for j in range(count):
        to = pl.multiple_of(j * at_ref[1] + index * at_ref[2], chunk)
        put(pl.ds(to, chunk), source(slice(j * chunk, (j + 1) * chunk)))


def begin_body(at_ref, theirs_ref, mine_ref, *refs):
    *pieces, total_ref, picked_ref, down_ref, up_ref = refs
    count = len(pieces) + 1
    units = total_ref.shape[1]
    block = picked_ref.shape[1]
    chunk = block // count
    height = mine_ref.shape[0]
    blank = jnp.zeros((chunk, units), up_ref.dtype)
    for r in range(count):
        if r == count // 2:
            place(at_ref, r, count, chunk, lambda _: blank, up_ref.__setitem__)
            continue
        piece = pieces[r if r < count // 2 else r - 1]
        place(at_ref, r, count, chunk, lambda rows: piece[rows, :units], up_ref.__setitem__)
        place(at_ref, r, count, chunk, lambda rows: piece[rows, units:], down_ref.__setitem__)
    index = lax.rem(at_ref[0] + count // 2, count)
    row = lax.broadcasted_iota(jnp.int32, (up_ref.shape[0], block), 0)
    col = lax.broadcasted_iota(jnp.int32, (up_ref.shape[0], block), 1)
    wanted = (col // chunk) * at_ref[1] + col % chunk + index * at_ref[2]
    pick = jnp.where(row == wanted, 1.0, 0.0).astype(jnp.bfloat16)
    for i, rows_ref in enumerate((theirs_ref, mine_ref)):
        rows = rows_ref[...]
        span = slice(i * height, (i + 1) * height)
        total_ref[span] = jnp.dot(rows, up_ref[...], preferred_element_type=jnp.float32)
        picked_ref[span] = jnp.dot(rows, pick, preferred_element_type=jnp.float32).astype(
            jnp.bfloat16
        )


def begin(at, theirs, mine, pieces):
    height, width = mine.shape
    block, units = pieces[0].shape[0], pieces[0].shape[1] // 2
    smem = pl.BlockSpec(memory_space=pltpu.SMEM)
    vmem = pl.BlockSpec(memory_space=pltpu.VMEM)
    return pl.pallas_call(
        begin_body,
        in_specs=[smem] + [vmem] * (2 + len(pieces)),
        out_specs=[vmem] * 3,
        out_shape=[
            pltpu.VMEM((2 * height, units), jnp.float32),
            pltpu.VMEM((2 * height, block), jnp.bfloat16),
            pltpu.VMEM((width, units), jnp.bfloat16),
        ],
        scratch_shapes=[pltpu.VMEM((width, units), jnp.bfloat16)],
        cost_estimate=pl.CostEstimate(flops=1 << 31, transcendentals=0, bytes_accessed=1 << 23),
        compiler_params=pltpu.CompilerParams(vmem_limit_bytes=36 << 20),
        name="begin",
    )(at, theirs, mine, *pieces)


def mixer_body(at_ref, total_ref, picked_ref, first_ref, second_ref, _, act_ref, out_ref, down_ref):
    units = act_ref.shape[1]
    block = picked_ref.shape[1]
    height, width = out_ref.shape
    count = width // block
    last = jnp.concatenate([first_ref[...], second_ref[...]], axis=0)
    place(
        at_ref, count // 2, count, block // count, lambda rows: last[rows, units:],
        down_ref.__setitem__,
    )
    wide = total_ref[...] + jnp.dot(
        picked_ref[...], last[:, :units], preferred_element_type=jnp.float32
    )
    act = jnp.square(jnp.maximum(wide, 0.0)).astype(jnp.bfloat16)
    act_ref[...] = act[height:]
    out_ref[...] = lax.dot_general(
        act[:height], down_ref[...], (((1,), (1,)), ((), ())), preferred_element_type=jnp.float32
    ).astype(out_ref.dtype)


def mixer(at, total, picked, first, second, down_t):
    width, units = down_t.shape
    height = total.shape[0] // 2
    smem = pl.BlockSpec(memory_space=pltpu.SMEM)
    vmem = pl.BlockSpec(memory_space=pltpu.VMEM)
    return pl.pallas_call(
        mixer_body,
        in_specs=[smem] + [vmem] * 5,
        out_specs=[vmem] * 3,
        out_shape=[
            pltpu.VMEM((height, units), jnp.bfloat16),
            pltpu.VMEM((height, width), jnp.bfloat16),
            pltpu.VMEM((width, units), jnp.bfloat16),
        ],
        input_output_aliases={5: 2},
        cost_estimate=pl.CostEstimate(flops=1 << 30, transcendentals=0, bytes_accessed=1 << 22),
        compiler_params=pltpu.CompilerParams(vmem_limit_bytes=32 << 20),
        name="mixer",
    )(at, total, picked, first, second, down_t)


def attention_body(
    core_ref, slope_ref, sink_ref, q_ref, kt_ref, vt_ref, doc_ref, before_ref, after_ref,
    qg_ref, kg_ref, other_ref, own_ref, kn_ref, vn_ref, dk_ref
):
    head = kt_ref.shape[0]
    heads = q_ref.shape[1] // head
    kg = kg_ref[...]
    for j in range(6):
        if j == 0:
            kt, vt, doc = before_ref[:head, :], before_ref[head : 2 * head, :], before_ref[2 * head : 2 * head + 8, :]
        elif j == 5:
            kt, vt, doc = after_ref[:head, :], after_ref[head : 2 * head, :], after_ref[2 * head : 2 * head + 8, :]
        else:
            lanes = slice((j - 1) * WINDOW, j * WINDOW)
            kt, vt, doc = kt_ref[:, lanes], vt_ref[:, lanes], doc_ref[:8, lanes]
        wide = kt.astype(jnp.float32)
        scale = lax.rsqrt(jnp.mean(wide * wide, axis=0, keepdims=True) + EPS)
        kn_ref[j] = (wide * scale * kg).astype(jnp.bfloat16)
        vn_ref[j] = vt
        dk_ref[j] = doc.astype(jnp.float32)
    row = lax.broadcasted_iota(jnp.int32, (WINDOW, 3 * WINDOW), 0)
    col = lax.broadcasted_iota(jnp.int32, (WINDOW, 3 * WINDOW), 1)
    distance = jnp.abs(col - WINDOW - row)
    near = distance <= WINDOW
    far = distance.astype(jnp.float32)
    core = core_ref[0]
    for half in range(2):
        side = 1 - core if half == 0 else core
        for j in range(2):
            block = 2 * side + j
            q = q_ref[pl.ds(pl.multiple_of(block * WINDOW, WINDOW), WINDOW), :]
            keys = jnp.concatenate([kn_ref[block], kn_ref[block + 1], kn_ref[block + 2]], axis=1)
            vals = jnp.concatenate([vn_ref[block], vn_ref[block + 1], vn_ref[block + 2]], axis=1)
            doc_k = jnp.concatenate(
                [jnp.broadcast_to(dk_ref[block + i][:1], (WINDOW, WINDOW)) for i in range(3)], axis=1
            )
            doc_q = jnp.broadcast_to(dk_ref[block + 1][:1], (WINDOW, WINDOW)).T
            allowed = near & (doc_k == jnp.concatenate([doc_q] * 3, axis=1))
            outs = []
            for h in range(heads):
                wide = q[:, h * head : (h + 1) * head].astype(jnp.float32)
                scale = lax.rsqrt(jnp.mean(wide * wide, axis=-1, keepdims=True) + EPS)
                qn = (wide * scale * qg_ref[...]).astype(jnp.bfloat16)
                s = jnp.dot(qn, keys, preferred_element_type=jnp.float32) * head ** (-0.5)
                s = jnp.where(allowed, s - slope_ref[h] * far, jnp.float32(-1e30))
                top = jnp.maximum(jnp.max(s, axis=-1, keepdims=True), sink_ref[h])
                p = jnp.exp(s - top)
                denom = jnp.sum(p, axis=-1, keepdims=True) + jnp.exp(sink_ref[h] - top)
                mixed = lax.dot_general(
                    p.astype(jnp.bfloat16), vals, (((1,), (1,)), ((), ())),
                    preferred_element_type=jnp.float32,
                )
                outs.append((mixed / denom).astype(jnp.bfloat16))
            target = other_ref if half == 0 else own_ref
            target[j * WINDOW : (j + 1) * WINDOW, :] = jnp.concatenate(outs, axis=1)


def attention(core, slopes, sink, q, kt, vt, doc, before, after, q_gain, k_gain):
    head, rows = kt.shape
    smem = pl.BlockSpec(memory_space=pltpu.SMEM)
    vmem = pl.BlockSpec(memory_space=pltpu.VMEM)
    out = pltpu.VMEM((rows // 2, q.shape[1]), jnp.bfloat16)
    return pl.pallas_call(
        attention_body,
        in_specs=[smem] * 3 + [vmem] * 8,
        out_specs=[vmem, vmem],
        out_shape=[out, out],
        scratch_shapes=[
            pltpu.VMEM((6, head, WINDOW), jnp.bfloat16),
            pltpu.VMEM((6, head, WINDOW), jnp.bfloat16),
            pltpu.VMEM((6, 8, WINDOW), jnp.float32),
        ],
        cost_estimate=pl.CostEstimate(flops=1 << 31, transcendentals=1 << 20, bytes_accessed=1 << 20),
        name="attend",
    )(core, slopes, sink, q, kt, vt, doc, before, after, q_gain, k_gain)


def shards(
    resid, queries, keys, values, documents, q_gain, k_gain, sink, w_out, n_gain, w_up, w_down
):
    rows = resid.shape[0]
    heads_here = sink.shape[0]
    core = lax.axis_index("c")
    half = rows // 2
    share = rows // lax.axis_size(TP)
    nx = lax.axis_size("x")

    kt, vt = keys.T, values.T
    doc = jnp.broadcast_to((documents + 1).astype(jnp.bfloat16)[None, :], (16, rows))
    packed = jnp.concatenate([kt, vt, doc], axis=0)
    count = lax.axis_size(SP)
    onward = [(i, i + 1) for i in range(count - 1)]
    before = lax.ppermute(packed[:, rows - WINDOW :], SP, onward)
    after = lax.ppermute(packed[:, :WINDOW], SP, [(j, i) for i, j in onward])
    piece = across(copies_of(w_up, w_down.T, lax.axis_size("z")))
    w_out_other = swap(w_out)

    heads_all = heads_here * lax.axis_size(TP)
    first_head = (lax.axis_index(TP) * heads_here).astype(jnp.float32)
    slopes = jnp.exp2(
        -8.0 * (first_head + jnp.arange(heads_here, dtype=jnp.float32) + 1.0) / heads_all
    )
    att_send, att_own = attention(
        core.astype(jnp.int32).reshape(1), slopes, sink, queries, kt, vt, doc, before, after,
        q_gain[None, :], k_gain[:, None],
    )
    cut = piece.shape[0] // 2
    up1, dn1 = along(piece, 1), along(piece, -1)
    up2, dn2 = along(up1, 1), along(dn1, -1)
    up3, dn3 = along(up2, 1), along(dn2, -1)
    up4, dn4 = along(up2[:cut], 2), along(dn2[cut:], -2)
    pieces = [piece, dn1, dn2, dn3, up3, up2, up1]

    att_other = swap(att_send)
    partial = jnp.dot(att_own, w_out, preferred_element_type=jnp.float32) + jnp.dot(
        att_other, w_out_other, preferred_element_type=jnp.float32
    )
    tiles = lax.all_to_all(
        partial.astype(jnp.bfloat16).reshape(nx, share, -1), "x", 0, 0, tiled=True
    )
    head_mix = jnp.sum(tiles.astype(jnp.float32), axis=0)
    start = core * half + lax.axis_index("x") * share
    own_resid = lax.dynamic_slice_in_dim(resid, start, share, 0)
    middle = (own_resid.astype(jnp.float32) + head_mix).astype(jnp.bfloat16)
    normed = rms_scale(middle, n_gain).astype(jnp.bfloat16)
    mine = spread(normed, "x")
    theirs = swap(mine)
    z, y = lax.axis_index("z"), lax.axis_index("y")
    chunk, block = w_up.shape[0], w_up.shape[0] * lax.axis_size("y")
    at = jnp.stack(
        [jnp.where(core == 0, y, z), jnp.where(core == 0, block, chunk), jnp.where(core == 0, chunk, block)]
    ).astype(jnp.int32)
    total, picked, down_t = begin(at, theirs, mine, pieces)
    active, out, down_t = mixer(at, total, picked, up4, dn4, down_t)
    sent = swap(out)
    kept = lax.optimization_barrier(
        lax.dot_general(
            active, down_t, (((1,), (1,)), ((), ())), preferred_element_type=jnp.float32
        )
    )
    joined = (kept + sent.astype(jnp.float32)).astype(jnp.bfloat16)
    unit_mix = scatter_x(joined)
    finished = spread((middle.astype(jnp.float32) + unit_mix).astype(jnp.bfloat16), "x")
    finished_other = swap(finished)
    out = lax.dynamic_update_slice_in_dim(
        jnp.zeros(resid.shape, resid.dtype), finished, core * half, 0
    )
    out = lax.optimization_barrier(out)
    return lax.dynamic_update_slice_in_dim(out, finished_other, (1 - core) * half, 0)


def solution(mesh):
    fine = Mesh(mesh.devices.reshape(8, 8, 4, 2), ("z", "y", "x", "c"))
    placed = (
        P(SP, None),
        P(SP, TP),
        P(SP, TP),
        P(SP, TP),
        P(SP),
        P(),
        P(),
        P(TP),
        P(TP, None),
        P(),
        P(SP, TP),
        P(TP, SP),
    )
    return jax.shard_map(shards, mesh=fine, in_specs=placed, out_specs=P(SP, None), check_vma=False)
```

```python
import jax
import jax.numpy as jnp
from jax import lax
from jax.experimental import pallas as pl
from jax.experimental.pallas import tpu as pltpu
from jax.sharding import Mesh
from jax.sharding import PartitionSpec as P

WINDOW = 128
EPS = 1e-06
SP = ("z", "y")
TP = ("x", "c")


def along(x, by):
    nz, ny = lax.axis_size("z"), lax.axis_size("y")
    pairs = []
    for z in range(nz):
        for y in range(ny):
            here = 2 * (z * ny + y)
            pairs.append((here, 2 * (z * ny + (y + by) % ny)))
            pairs.append((here + 1, 2 * ((z + by) % nz * ny + y) + 1))
    return lax.ppermute(x, ("z", "y", "c"), pairs)


def across(copies):
    nz, ny = lax.axis_size("z"), lax.axis_size("y")
    groups = [[2 * (z * ny + y) for z in range(nz)] for y in range(ny)]
    groups += [[2 * (z * ny + y) + 1 for y in range(ny)] for z in range(nz)]
    tiles = lax.all_to_all(
        copies, ("z", "y", "c"), 0, 0, tiled=True, axis_index_groups=groups
    )
    return tiles.reshape(-1, tiles.shape[2])


def swap(x):
    return lax.ppermute(x, "c", [(0, 1), (1, 0)])


def spread(x, axis):
    n = lax.axis_size(axis)
    tiles = lax.all_to_all(jnp.broadcast_to(x, (n, *x.shape)), axis, 0, 0, tiled=True)
    return tiles.reshape(n * x.shape[0], x.shape[1])


def copies_body(up_ref, down_ref, out_ref):
    units = up_ref.shape[1]
    for i in range(out_ref.shape[0]):
        out_ref[i, :, :units] = up_ref[...]
        out_ref[i, :, units:] = down_ref[...]


def copies_of(up, down_t, count):
    rows, units = up.shape
    vmem = pl.BlockSpec(memory_space=pltpu.VMEM)
    return pl.pallas_call(
        copies_body,
        in_specs=[vmem, vmem],
        out_specs=vmem,
        out_shape=pltpu.VMEM((count, rows, 2 * units), up.dtype),
        name="copies",
    )(up, down_t)


def scatter_x(x):
    n = lax.axis_size("x")
    tiles = lax.all_to_all(x.reshape(n, x.shape[0] // n, x.shape[1]), "x", 0, 0, tiled=True)
    return jnp.sum(tiles.astype(jnp.float32), axis=0)


def rms_scale(field, gain):
    wide = field.astype(jnp.float32)
    return wide * lax.rsqrt(jnp.mean(wide * wide, axis=-1, keepdims=True) + EPS) * gain


def place(at_ref, r, count, chunk, source, put):
    index = lax.rem(at_ref[0] + r, count)
    for j in range(count):
        to = pl.multiple_of(j * at_ref[1] + index * at_ref[2], chunk)
        put(pl.ds(to, chunk), source(slice(j * chunk, (j + 1) * chunk)))


def begin_body(at_ref, theirs_ref, mine_ref, *refs):
    *pieces, total_ref, picked_ref, down_ref, up_ref = refs
    count = len(pieces) + 1
    units = total_ref.shape[1]
    block = picked_ref.shape[1]
    chunk = block // count
    height = mine_ref.shape[0]
    blank = jnp.zeros((chunk, units), up_ref.dtype)
    for r in range(count):
        if r == count // 2:
            place(at_ref, r, count, chunk, lambda _: blank, up_ref.__setitem__)
            continue
        piece = pieces[r if r < count // 2 else r - 1]
        place(at_ref, r, count, chunk, lambda rows: piece[rows, :units], up_ref.__setitem__)
        place(at_ref, r, count, chunk, lambda rows: piece[rows, units:], down_ref.__setitem__)
    index = lax.rem(at_ref[0] + count // 2, count)
    row = lax.broadcasted_iota(jnp.int32, (up_ref.shape[0], block), 0)
    col = lax.broadcasted_iota(jnp.int32, (up_ref.shape[0], block), 1)
    wanted = (col // chunk) * at_ref[1] + col % chunk + index * at_ref[2]
    pick = jnp.where(row == wanted, 1.0, 0.0).astype(jnp.bfloat16)
    for i, rows_ref in enumerate((theirs_ref, mine_ref)):
        rows = rows_ref[...]
        span = slice(i * height, (i + 1) * height)
        total_ref[span] = jnp.dot(rows, up_ref[...], preferred_element_type=jnp.float32)
        picked_ref[span] = jnp.dot(rows, pick, preferred_element_type=jnp.float32).astype(
            jnp.bfloat16
        )


def begin(at, theirs, mine, pieces):
    height, width = mine.shape
    block, units = pieces[0].shape[0], pieces[0].shape[1] // 2
    smem = pl.BlockSpec(memory_space=pltpu.SMEM)
    vmem = pl.BlockSpec(memory_space=pltpu.VMEM)
    return pl.pallas_call(
        begin_body,
        in_specs=[smem] + [vmem] * (2 + len(pieces)),
        out_specs=[vmem] * 3,
        out_shape=[
            pltpu.VMEM((2 * height, units), jnp.float32),
            pltpu.VMEM((2 * height, block), jnp.bfloat16),
            pltpu.VMEM((width, units), jnp.bfloat16),
        ],
        scratch_shapes=[pltpu.VMEM((width, units), jnp.bfloat16)],
        cost_estimate=pl.CostEstimate(flops=1 << 31, transcendentals=0, bytes_accessed=1 << 23),
        compiler_params=pltpu.CompilerParams(vmem_limit_bytes=36 << 20),
        name="begin",
    )(at, theirs, mine, *pieces)


def mixer_body(at_ref, total_ref, picked_ref, first_ref, second_ref, _, act_ref, out_ref, down_ref):
    units = act_ref.shape[1]
    block = picked_ref.shape[1]
    height, width = out_ref.shape
    count = width // block
    last = jnp.concatenate([first_ref[...], second_ref[...]], axis=0)
    place(
        at_ref, count // 2, count, block // count, lambda rows: last[rows, units:],
        down_ref.__setitem__,
    )
    wide = total_ref[...] + jnp.dot(
        picked_ref[...], last[:, :units], preferred_element_type=jnp.float32
    )
    act = jnp.square(jnp.maximum(wide, 0.0)).astype(jnp.bfloat16)
    act_ref[...] = act[height:]
    out_ref[...] = lax.dot_general(
        act[:height], down_ref[...], (((1,), (1,)), ((), ())), preferred_element_type=jnp.float32
    ).astype(out_ref.dtype)


def mixer(at, total, picked, first, second, down_t):
    width, units = down_t.shape
    height = total.shape[0] // 2
    smem = pl.BlockSpec(memory_space=pltpu.SMEM)
    vmem = pl.BlockSpec(memory_space=pltpu.VMEM)
    return pl.pallas_call(
        mixer_body,
        in_specs=[smem] + [vmem] * 5,
        out_specs=[vmem] * 3,
        out_shape=[
            pltpu.VMEM((height, units), jnp.bfloat16),
            pltpu.VMEM((height, width), jnp.bfloat16),
            pltpu.VMEM((width, units), jnp.bfloat16),
        ],
        input_output_aliases={5: 2},
        cost_estimate=pl.CostEstimate(flops=1 << 30, transcendentals=0, bytes_accessed=1 << 22),
        compiler_params=pltpu.CompilerParams(vmem_limit_bytes=32 << 20),
        name="mixer",
    )(at, total, picked, first, second, down_t)


def attend_blocks(inner, core_ref, slope_ref, sink_ref, q_ref, key_blocks, qg_ref, kg_ref, put, kn_ref, vn_ref, dk_ref):
    head = kn_ref.shape[1]
    heads = q_ref.shape[1] // head
    kg = jnp.broadcast_to(kg_ref[...], (WINDOW, head)).T
    for j, (kt, vt, doc) in key_blocks:
        wide = kt.astype(jnp.float32)
        scale = lax.rsqrt(jnp.mean(wide * wide, axis=0, keepdims=True) + EPS)
        kn_ref[j] = (wide * scale * kg).astype(jnp.bfloat16)
        vn_ref[j] = vt
        dk_ref[j] = doc.astype(jnp.float32)
    row = lax.broadcasted_iota(jnp.int32, (WINDOW, 3 * WINDOW), 0)
    col = lax.broadcasted_iota(jnp.int32, (WINDOW, 3 * WINDOW), 1)
    distance = jnp.abs(col - WINDOW - row)
    near = distance <= WINDOW
    far = distance.astype(jnp.float32)
    core = core_ref[0]
    for half in range(2):
        side = 1 - core if half == 0 else core
        block = 1 + side if inner else 3 * side
        q = q_ref[pl.ds(pl.multiple_of(block * WINDOW, WINDOW), WINDOW), :]
        keys = jnp.concatenate([kn_ref[block], kn_ref[block + 1], kn_ref[block + 2]], axis=1)
        vals = jnp.concatenate([vn_ref[block], vn_ref[block + 1], vn_ref[block + 2]], axis=1)
        doc_k = jnp.concatenate(
            [jnp.broadcast_to(dk_ref[block + i][:1], (WINDOW, WINDOW)) for i in range(3)], axis=1
        )
        doc_q = jnp.broadcast_to(dk_ref[block + 1][:1], (WINDOW, WINDOW)).T
        allowed = near & (doc_k == jnp.concatenate([doc_q] * 3, axis=1))
        outs = []
        for h in range(heads):
            wide = q[:, h * head : (h + 1) * head].astype(jnp.float32)
            scale = lax.rsqrt(jnp.mean(wide * wide, axis=-1, keepdims=True) + EPS)
            qn = (wide * scale * qg_ref[...]).astype(jnp.bfloat16)
            s = jnp.dot(qn, keys, preferred_element_type=jnp.float32) * head ** (-0.5)
            s = jnp.where(allowed, s - slope_ref[h] * far, jnp.float32(-1e30))
            top = jnp.maximum(jnp.max(s, axis=-1, keepdims=True), sink_ref[h])
            p = jnp.exp(s - top)
            denom = jnp.sum(p, axis=-1, keepdims=True) + jnp.exp(sink_ref[h] - top)
            mixed = lax.dot_general(
                p.astype(jnp.bfloat16), vals, (((1,), (1,)), ((), ())),
                preferred_element_type=jnp.float32,
            )
            outs.append((mixed / denom).astype(jnp.bfloat16))
        put(half, side, jnp.concatenate(outs, axis=1))


def own_blocks(kt_ref, vt_ref, doc_ref):
    found = []
    for j in range(1, 5):
        lanes = slice((j - 1) * WINDOW, j * WINDOW)
        found.append((j, (kt_ref[:, lanes], vt_ref[:, lanes], doc_ref[:8, lanes])))
    return found


def inner_body(
    core_ref, slope_ref, sink_ref, q_ref, kt_ref, vt_ref, doc_ref, qg_ref, kg_ref,
    out_ref, kn_ref, vn_ref, dk_ref
):
    def put(half, side, value):
        out_ref[half] = value

    attend_blocks(
        True, core_ref, slope_ref, sink_ref, q_ref, own_blocks(kt_ref, vt_ref, doc_ref),
        qg_ref, kg_ref, put, kn_ref, vn_ref, dk_ref,
    )


def outer_body(
    core_ref, slope_ref, sink_ref, q_ref, kt_ref, vt_ref, doc_ref, qg_ref, kg_ref,
    before_ref, after_ref, inner_ref, other_ref, own_ref, kn_ref, vn_ref, dk_ref
):
    head = kt_ref.shape[0]

    def put(half, side, value):
        target = other_ref if half == 0 else own_ref
        target[pl.ds(pl.multiple_of(side * WINDOW, WINDOW), WINDOW), :] = value
        target[pl.ds(pl.multiple_of((1 - side) * WINDOW, WINDOW), WINDOW), :] = inner_ref[half]

    blocks = own_blocks(kt_ref, vt_ref, doc_ref)
    for j, ref in ((0, before_ref), (5, after_ref)):
        blocks.append((j, (ref[:head, :], ref[head : 2 * head, :], ref[2 * head : 2 * head + 8, :])))
    attend_blocks(
        False, core_ref, slope_ref, sink_ref, q_ref, blocks, qg_ref, kg_ref, put, kn_ref, vn_ref, dk_ref
    )


def attention(body, out_shape, core, slopes, sink, q, kt, vt, doc, q_gain, k_gain, *more):
    head = kt.shape[0]
    smem = pl.BlockSpec(memory_space=pltpu.SMEM)
    vmem = pl.BlockSpec(memory_space=pltpu.VMEM)
    return pl.pallas_call(
        body,
        in_specs=[smem] * 3 + [vmem] * (6 + len(more)),
        out_specs=[vmem] * len(out_shape),
        out_shape=out_shape,
        scratch_shapes=[
            pltpu.VMEM((6, head, WINDOW), jnp.bfloat16),
            pltpu.VMEM((6, head, WINDOW), jnp.bfloat16),
            pltpu.VMEM((6, 8, WINDOW), jnp.float32),
        ],
        cost_estimate=pl.CostEstimate(flops=1 << 30, transcendentals=1 << 19, bytes_accessed=1 << 20),
        compiler_params=pltpu.CompilerParams(vmem_limit_bytes=12 << 20),
    )(core, slopes, sink, q, kt, vt, doc, q_gain, k_gain, *more)


def shards(
    resid, queries, keys, values, documents, q_gain, k_gain, sink, w_out, n_gain, w_up, w_down
):
    rows = resid.shape[0]
    heads_here = sink.shape[0]
    core = lax.axis_index("c")
    half = rows // 2
    share = rows // lax.axis_size(TP)
    nx = lax.axis_size("x")

    kt, vt = keys.T, values.T
    doc = jnp.broadcast_to((documents + 1).astype(jnp.bfloat16)[None, :], (16, rows))
    packed = jnp.concatenate([kt, vt, doc], axis=0)
    count = lax.axis_size(SP)
    onward = [(i, i + 1) for i in range(count - 1)]
    before = lax.ppermute(packed[:, rows - WINDOW :], SP, onward)
    after = lax.ppermute(packed[:, :WINDOW], SP, [(j, i) for i, j in onward])
    piece = across(copies_of(w_up, w_down.T, lax.axis_size("z")))
    w_out_other = swap(w_out)

    heads_all = heads_here * lax.axis_size(TP)
    first_head = (lax.axis_index(TP) * heads_here).astype(jnp.float32)
    slopes = jnp.exp2(
        -8.0 * (first_head + jnp.arange(heads_here, dtype=jnp.float32) + 1.0) / heads_all
    )
    shared = (
        core.astype(jnp.int32).reshape(1), slopes, sink, queries, kt, vt, doc,
        q_gain[None, :], k_gain[None, :],
    )
    width = queries.shape[1]
    (inner,) = attention(
        inner_body, [pltpu.VMEM((2, WINDOW, width), jnp.bfloat16)], *shared
    )
    att_send, att_own = attention(
        outer_body, [pltpu.VMEM((half, width), jnp.bfloat16)] * 2, *shared, before, after, inner
    )
    cut = piece.shape[0] // 2
    up1, dn1 = along(piece, 1), along(piece, -1)
    up2, dn2 = along(up1, 1), along(dn1, -1)
    up3, dn3 = along(up2, 1), along(dn2, -1)
    up4, dn4 = along(up2[:cut], 2), along(dn2[cut:], -2)
    pieces = [piece, dn1, dn2, dn3, up3, up2, up1]

    att_other = swap(att_send)
    partial = jnp.dot(att_own, w_out, preferred_element_type=jnp.float32) + jnp.dot(
        att_other, w_out_other, preferred_element_type=jnp.float32
    )
    tiles = lax.all_to_all(
        partial.astype(jnp.bfloat16).reshape(nx, share, -1), "x", 0, 0, tiled=True
    )
    head_mix = jnp.sum(tiles.astype(jnp.float32), axis=0)
    start = core * half + lax.axis_index("x") * share
    own_resid = lax.dynamic_slice_in_dim(resid, start, share, 0)
    middle = (own_resid.astype(jnp.float32) + head_mix).astype(jnp.bfloat16)
    normed = rms_scale(middle, n_gain).astype(jnp.bfloat16)
    mine = spread(normed, "x")
    theirs = swap(mine)
    z, y = lax.axis_index("z"), lax.axis_index("y")
    chunk, block = w_up.shape[0], w_up.shape[0] * lax.axis_size("y")
    at = jnp.stack(
        [jnp.where(core == 0, y, z), jnp.where(core == 0, block, chunk), jnp.where(core == 0, chunk, block)]
    ).astype(jnp.int32)
    total, picked, down_t = begin(at, theirs, mine, pieces)
    active, out, down_t = mixer(at, total, picked, up4, dn4, down_t)
    sent = swap(out)
    kept = lax.optimization_barrier(
        lax.dot_general(
            active, down_t, (((1,), (1,)), ((), ())), preferred_element_type=jnp.float32
        )
    )
    joined = (kept + sent.astype(jnp.float32)).astype(jnp.bfloat16)
    unit_mix = scatter_x(joined)
    finished = spread((middle.astype(jnp.float32) + unit_mix).astype(jnp.bfloat16), "x")
    finished_other = swap(finished)
    out = lax.dynamic_update_slice_in_dim(
        jnp.zeros(resid.shape, resid.dtype), finished, core * half, 0
    )
    out = lax.optimization_barrier(out)
    return lax.dynamic_update_slice_in_dim(out, finished_other, (1 - core) * half, 0)


def solution(mesh):
    fine = Mesh(mesh.devices.reshape(8, 8, 4, 2), ("z", "y", "x", "c"))
    placed = (
        P(SP, None),
        P(SP, TP),
        P(SP, TP),
        P(SP, TP),
        P(SP),
        P(),
        P(),
        P(TP),
        P(TP, None),
        P(),
        P(SP, TP),
        P(TP, SP),
    )
    return jax.shard_map(shards, mesh=fine, in_specs=placed, out_specs=P(SP, None), check_vma=False)
```
